512 devices in a mesh: ep: 32 (over z, x), tp: 16 (over y, core).
Axes of the slice: x: 4, y: 8, z: 8, core: 2. Of those that a mesh axis runs over, the one named last changes fastest.
Arguments:
- tokens: bfloat16 [4096, 4096], P('ep', 'tp'), may hold values from -6 to 6
- cotangent: bfloat16 [4096, 4096], P('ep', 'tp'), may hold values from -6 to 6
- routes: int32 [4096, 2], P('ep'), may hold values from 0 to 31, all different within a row; in each aligned block of 128 rows (0 to 127, 128 to 255, ...) at most 12 rows name the same one
- gate_weight: float32 [4096, 2], P('ep'), may hold values from 0.1 to 2.5
- w_gate: bfloat16 [32, 1024, 4096], P('ep', 'tp'), may hold values from -0.09375 to 0.09375
- w_up: bfloat16 [32, 1024, 4096], P('ep', 'tp'), may hold values from -0.09375 to 0.09375
- w_down: bfloat16 [32, 1024, 4096], P('ep', 'tp'), may hold values from -0.1875 to 0.1875
- shared_hidden: bfloat16 [4096, 1024], P('ep'), may hold values from -4 to 4
Outputs:
- tokens_grad: bfloat16 [4096, 4096], P('ep', 'tp')
- gate_grad: float32 [4096, 2], P('ep')
- w_gate_grad: float32 [32, 1024, 4096], P('ep', 'tp')
- w_up_grad: float32 [32, 1024, 4096], P('ep', 'tp')
- w_down_grad: float32 [32, 1024, 4096], P('ep', 'tp')
- shared_grad: float32 [1024, 4096], P('ep', 'tp')
The draws below stay inside these ranges and needn't reach their ends.
Inputs may be any that keep to these rules, and one draw needn't show every extreme that they name: `routes`: each row names 2 different experts. Among the rows of one index of ep (aligned blocks of 128 rows) no expert is named more than 12 times, and in every draw some expert is named exactly 12 times in some block.
All inputs are finite; a program needn't handle non-finite values.
Results may differ from the reference program's by a relative error of at most 0.022.
Values may be sent and summed in bfloat16 or wider, within the bound.
No kernel may reach another device: no remote copies, remote signals or barrier semaphores. Data moves between devices by JAX's collectives and lax.ppermute only.
A program may use at most 64 MiB of HBM per device.

```python
import math
import jax
import jax.numpy as jnp
import numpy as np
from jax import lax

D = 4096
HIDDEN_SIZE = 1024
SHARED_HIDDEN = 1024
TOP_K = 2
TOK_DEV = 128
EXPERTS = 32
CAP = 12
TOKENS = 4096
N_EP = 32
N_TP = 16


def with_spikes(drawn, rng, source, target, parts, factor):
    def block_of(position):
        return (jnp.arange(drawn.shape[position]) // (drawn.shape[position] // parts)).reshape((-1,) + (1,) * (drawn.ndim - 1 - position))

    near = jax.random.permutation(rng, parts)[block_of(target)]
    second = (block_of(target) + parts // 2) % parts
    return jnp.where((block_of(source) == near) | (block_of(source) == second), factor * drawn, drawn)


def levels(rng, shape, pieces, low, largest):
    def one(axis_at, shards_of):
        heights = jax.random.uniform(jax.random.fold_in(jax.random.fold_in(rng, 6), axis_at), (shards_of,), jnp.float32, low / len(pieces), largest / len(pieces))
        return jnp.repeat(jnp.exp(heights), shape[axis_at] // shards_of).reshape((-1,) + (1,) * (len(shape) - axis_at - 1))

    level = one(*pieces[0])
    for cut in pieces[1:]:
        level = level * one(*cut)
    return level


def deal_out(rng, own, number, rows, count, top, bound, lean):
    ranking = jax.random.permutation(rng, count)
    packed, common = portions_of(count, rows * top, bound, lean, True), portions_of(count, rows * top, bound, lean, False)
    places = jnp.arange(count)

    def named(tallies, turn):
        used = int((tallies > 0).sum())
        fixed = max(1, used // 4)
        moved = fixed + (places - fixed + turn * (used - fixed)) % max(1, count - fixed)
        return jnp.zeros((count,), jnp.int32).at[ranking[jnp.where(places < fixed, places, moved)]].set(jnp.asarray(tallies, jnp.int32))

    tallies = jnp.where(number % 4 == 0, named(packed, number // 4), named(common, number - number // 4 - 1))
    mixed = jax.random.permutation(jax.random.fold_in(own, 3), count)
    giver, receiver = mixed[0:count // 2 * 2:2], mixed[1:count // 2 * 2:2]
    room = jnp.minimum(tallies[giver] - 1, bound - tallies[receiver]) // 2
    room = jnp.where((giver == ranking[0]) | (receiver == ranking[0]) | (tallies[receiver] == 0), 0, jnp.maximum(room, 0))
    moved = jax.random.randint(jax.random.fold_in(own, 4), (count // 2,), 0, 1 << 20) % (room + 1)
    tallies = tallies.at[giver].add(-moved).at[receiver].add(moved)
    items = jnp.searchsorted(jnp.cumsum(tallies), jnp.arange(rows * top), side="right").astype(jnp.int32)
    table = items.reshape(top, rows).T
    table = table[jax.random.permutation(jax.random.fold_in(own, 1), rows)]
    turn = jax.random.randint(jax.random.fold_in(own, 2), (rows, 1), 0, top)
    return jnp.take_along_axis(table, (jnp.arange(top)[None, :] + turn) % top, axis=1)


def portions_of(count, total, limit, slope, full):
    portions = [(1 << 20) // math.isqrt(grade ** slope) + 1 for grade in range(1, count + 1)]
    largest = limit if full else min(limit, max(-(-total // count), total * portions[0] // sum(portions)))
    least = 1 if total - largest >= count - 1 else 0
    holding, surplus = [largest] + [least] * (count - 1), total - largest - least * (count - 1)
    while surplus > 0:
        movable = [i for i in range(1, count) if holding[i] < largest] or [i for i in range(1, count) if holding[i] < limit]
        whole, left = sum([portions[i] for i in movable]), surplus
        for i in movable:
            extra = min(limit - holding[i], max(1, left * portions[i] // whole), surplus)
            holding[i] = holding[i] + extra
            surplus = surplus - extra
    return np.array(holding)


def centred(key, dims, spread, bound, split=(), kind=jnp.bfloat16):
    drawn = spread * jax.random.normal(key, dims, jnp.float32)
    if split:
        drawn = drawn * levels(key, dims, split, -0.22, 0.18)
    return jnp.clip(drawn, -bound, bound).astype(kind)


def bell_draw_with(stream_key, extent, spread, most, cuts, heavy, kind=jnp.bfloat16):
    drawn = spread * jax.random.normal(stream_key, extent, jnp.float32)
    if cuts:
        drawn = drawn * levels(stream_key, extent, cuts, -0.22, 0.18)
    return jnp.clip(with_spikes(drawn, jax.random.fold_in(stream_key, 3), *heavy), -most, most).astype(kind)


def setup_inputs(seed: int = 0) -> dict:
    key_list = jax.random.split(jax.random.key(seed), 9)
    tokens = centred(key_list[0], (TOKENS, D), 1.0, 6.0, ((0, 32), (1, 16)))
    cotangent = centred(key_list[1], (TOKENS, D), 1.0, 6.0, ((0, 32), (1, 16)))
    routes_keys = jax.random.split(jax.random.fold_in(key_list[2], 1), TOKENS // TOK_DEV)
    routes_turns = jax.random.permutation(jax.random.fold_in(key_list[2], 3), TOKENS // TOK_DEV)
    routes = jax.vmap(lambda own, number: deal_out(jax.random.fold_in(key_list[2], 2), own, number, TOK_DEV, EXPERTS, TOP_K, CAP, 2))(routes_keys, routes_turns).reshape((TOKENS, TOP_K))
    gate_weight = jnp.clip(jnp.exp(math.log(2.5) - 3.218876 * jax.random.uniform(key_list[3], (TOKENS, TOP_K), jnp.float32) ** levels(key_list[3], (TOKENS, TOP_K), ((0, 32),), -0.2, 0.2)), 0.1, 2.5)
    w_gate = centred(key_list[4], (EXPERTS, HIDDEN_SIZE, D), D ** -0.5, 0.09375, ((0, 32), (1, 16)))
    w_up = centred(key_list[5], (EXPERTS, HIDDEN_SIZE, D), D ** -0.5, 0.09375, ((0, 32), (1, 16)))
    w_down = centred(key_list[6], (EXPERTS, HIDDEN_SIZE, D), HIDDEN_SIZE ** -0.5, 0.1875, ((0, 32), (1, 16)))
    shared_hidden = bell_draw_with(key_list[7], (TOKENS, SHARED_HIDDEN), 0.5, 4.0, ((0, 32),), (0, 1, 32, 2.75))
    return {"tokens": tokens, "cotangent": cotangent, "routes": routes, "gate_weight": gate_weight, "w_gate": w_gate, "w_up": w_up, "w_down": w_down, "shared_hidden": shared_hidden}


def slot_positions(device_routes):
    flat_routes = device_routes.reshape(-1)
    onehot = (flat_routes[:, None] == jnp.arange(EXPERTS, dtype=jnp.int32)[None, :]).astype(jnp.int32)
    earlier = jnp.cumsum(onehot, axis=0) - onehot
    return flat_routes, jnp.sum(earlier * onehot, axis=1).astype(jnp.int32)


def reference(tokens, cotangent, routes, gate_weight, w_gate, w_up, w_down, shared_hidden):
    assigned = TOK_DEV * TOP_K
    flat_routes, positions = jax.vmap(slot_positions)(routes.reshape(N_EP, assigned))
    sources = jnp.broadcast_to(jnp.arange(N_EP, dtype=jnp.int32)[:, None], (N_EP, assigned))
    token_ids = sources * TOK_DEV + jnp.arange(assigned, dtype=jnp.int32)[None, :] // TOP_K
    slot_table = jnp.full((EXPERTS, N_EP, CAP), TOKENS, jnp.int32).at[flat_routes, sources, positions].set(token_ids)
    weight_table = jnp.zeros((EXPERTS, N_EP, CAP), jnp.float32).at[flat_routes, sources, positions].set(
        gate_weight.reshape(N_EP, assigned))
    padded_tokens = jnp.concatenate([tokens, jnp.zeros((1, D), jnp.bfloat16)], 0)
    padded_cotan = jnp.concatenate([cotangent, jnp.zeros((1, D), jnp.bfloat16)], 0)
    groups = HIDDEN_SIZE // N_TP
    contract_last = (((1,), (1,)), ((), ()))

    def expert_fn(inputs):
        table_rows, weight_rows, gate_mat, up_mat, down_mat = inputs
        rows_x = padded_tokens[table_rows.reshape(-1)]
        rows_g = padded_cotan[table_rows.reshape(-1)]
        weight_col = weight_rows.reshape(-1, 1)
        pre_gate = lax.dot_general(rows_x, gate_mat, contract_last, preferred_element_type=jnp.float32)
        pre_up = lax.dot_general(rows_x, up_mat, contract_last, preferred_element_type=jnp.float32)
        sigmoid_gate = jax.nn.sigmoid(pre_gate)
        silu_gate = pre_gate * sigmoid_gate
        hidden = (silu_gate * pre_up).astype(jnp.bfloat16)
        back_hidden = lax.dot_general(rows_g, down_mat, contract_last, preferred_element_type=jnp.float32)
        gate_part = jnp.sum(hidden.astype(jnp.float32) * back_hidden, axis=1)
        scaled = weight_col * back_hidden
        grad_pre_gate = (scaled * pre_up * sigmoid_gate * (1.0 + pre_gate * (1.0 - sigmoid_gate))).astype(jnp.bfloat16)
        grad_pre_up = (scaled * silu_gate).astype(jnp.bfloat16)
        weighted_cotan = (weight_col * rows_g.astype(jnp.float32)).astype(jnp.bfloat16)
        grad_down = jnp.dot(hidden.T, weighted_cotan, preferred_element_type=jnp.float32)
        grad_gate = jnp.dot(grad_pre_gate.T, rows_x, preferred_element_type=jnp.float32)
        grad_up = jnp.dot(grad_pre_up.T, rows_x, preferred_element_type=jnp.float32)
        row_total = rows_x.shape[0]
        partial_value = jnp.einsum('rnh,nhd->nrd', grad_pre_gate.astype(jnp.float32).reshape(row_total, N_TP, groups),
                             gate_mat.astype(jnp.float32).reshape(N_TP, groups, D))
        partial_value = partial_value + jnp.einsum('rnh,nhd->nrd', grad_pre_up.astype(jnp.float32).reshape(row_total, N_TP, groups),
                                       up_mat.astype(jnp.float32).reshape(N_TP, groups, D))
        rounded = lax.optimization_barrier(partial_value.astype(jnp.bfloat16)).astype(jnp.float32)
        row_grad = jnp.sum(rounded, axis=0).astype(jnp.bfloat16)
        return row_grad.reshape(N_EP, CAP, D), gate_part.reshape(N_EP, CAP), grad_gate, grad_up, grad_down

    row_grads, gate_parts, w_gate_grad, w_up_grad, w_down_grad = lax.map(
        expert_fn, (slot_table, weight_table, w_gate, w_up, w_down))
    picked = row_grads[flat_routes, sources, positions].astype(jnp.float32)
    tokens_grad = jnp.sum(picked.reshape(TOKENS, TOP_K, D), axis=1).astype(jnp.bfloat16)
    gate_grad = gate_parts[flat_routes, sources, positions].reshape(TOKENS, TOP_K)
    shared_grad = jnp.dot(shared_hidden.T, cotangent, preferred_element_type=jnp.float32)
    return (tokens_grad, gate_grad, w_gate_grad, w_up_grad, w_down_grad, shared_grad)
```

```python
import jax
import jax.numpy as jnp
from jax import lax
from jax.experimental import pallas as pl
from jax.experimental.pallas import tpu as pltpu
from jax.sharding import Mesh, PartitionSpec as P

TOK, TOP, EXPERTS, CAP = 128, 2, 32, 12
SLOTS = EXPERTS * CAP
ROWS = 2 * SLOTS
PAIR = 2 * CAP
WIDTH = 256
NY = 8
HALF = NY * WIDTH
HID = 64
BACK = SLOTS + 16
EP = ("z", "x")
F32, BF16, I32 = jnp.float32, jnp.bfloat16, jnp.int32


def iota(shape, dim):
    return lax.broadcasted_iota(I32, shape, dim)


def slot_codes(rt):
    ids = iota((EXPERTS, TOK), 0)
    first, second = rt[0:1, :] == ids, rt[1:2, :] == ids
    hot = jnp.where(first, 1.0, 0.0) + jnp.where(second, 1.0, 0.0)
    upper = jnp.where(iota((TOK, TOK), 0) < iota((TOK, TOK), 1), 1.0, 0.0)
    rank = jnp.dot(hot.astype(BF16), upper.astype(BF16), preferred_element_type=F32)
    return jnp.where(hot > 0.5, rank, -1.0), first, second


def dispatch_kernel(rt_ref, gw_ref, tok_ref, cot_ref, out_ref):
    code, first, second = slot_codes(rt_ref[...])
    gw = gw_ref[...]
    weight = jnp.where(first, gw[0:1, :], 0.0) + jnp.where(second, gw[1:2, :], 0.0)
    shape = (EXPERTS, PAIR, TOK)
    code3 = jnp.broadcast_to(code[:, None, :], shape)
    weight3 = jnp.broadcast_to(weight[:, None, :], shape)
    at = iota(shape, 1)
    atf = at.astype(F32)
    sel_x = jnp.where(code3 == atf, jnp.where(at < CAP, 1.0, 0.0), 0.0)
    sel_g = jnp.where(code3 == atf - float(CAP), jnp.where(at >= CAP, 1.0, 0.0), 0.0)
    scale = jnp.sum(sel_g * weight3 + sel_x, axis=2, keepdims=True).reshape(ROWS, 1)
    select = jnp.concatenate(
        [sel_x.reshape(ROWS, TOK).astype(BF16), sel_g.reshape(ROWS, TOK).astype(BF16)], axis=1
    )
    source = jnp.concatenate([tok_ref[...], cot_ref[...]], axis=0)
    rows = jnp.dot(select, source, preferred_element_type=F32)
    out_ref[...] = (rows * scale).astype(BF16).reshape(EXPERTS, PAIR, WIDTH)


def dispatch(rt, gw, tokens, cotangent):
    return pl.pallas_call(
        dispatch_kernel,
        out_shape=jax.ShapeDtypeStruct((EXPERTS, PAIR, WIDTH), BF16),
        name="dispatch",
    )(rt, gw, tokens, cotangent)


def split_kernel(c_ref, wg_ref, wu_ref, wd_ref, out_ref):
    off = pl.multiple_of((1 - c_ref[0]) * WIDTH, WIDTH)
    out_ref[0] = wg_ref[:, pl.ds(off, WIDTH)]
    out_ref[1] = wu_ref[:, pl.ds(off, WIDTH)]
    out_ref[2] = wd_ref[:, pl.ds(off, WIDTH)]


def weight_spec():
    return pl.BlockSpec((HID, 2 * WIDTH), lambda i: (0, i))


def scalar_spec():
    return pl.BlockSpec(memory_space=pltpu.SMEM)


def whole(shape):
    return pl.BlockSpec(shape, lambda i: (0,) * len(shape))


def other_half(core, wg, wu, wd):
    return pl.pallas_call(
        split_kernel,
        grid=(NY,),
        in_specs=[scalar_spec()] + [weight_spec()] * 3,
        out_specs=pl.BlockSpec((3, HID, WIDTH), lambda i: (0, 0, i)),
        out_shape=jax.ShapeDtypeStruct((3, HID, HALF), BF16),
        name="other_half",
    )(core, wg, wu, wd)


def forward_kernel(c_ref, xg_ref, wg_ref, wu_ref, wd_ref, wr_ref, out_ref, acc_ref):
    step = pl.program_id(0)
    off = pl.multiple_of(c_ref[0] * WIDTH, WIDTH)
    mats = jnp.concatenate(
        [
            wg_ref[:, pl.ds(off, WIDTH)],
            wr_ref[0],
            wu_ref[:, pl.ds(off, WIDTH)],
            wr_ref[1],
            wd_ref[:, pl.ds(off, WIDTH)],
            wr_ref[2],
        ],
        axis=0,
    )
    part = lax.dot_general(
        xg_ref[0], mats, (((1,), (1,)), ((), ())), preferred_element_type=F32
    )

    @pl.when(step == 0)
    def _():
        acc_ref[...] = part

    @pl.when(step > 0)
    def _():
        acc_ref[...] = acc_ref[...] + part

    @pl.when(step == NY - 1)
    def _():
        for s in range(EXPERTS):
            out_ref[s * CAP : (s + 1) * CAP, 0 : 4 * HID] = acc_ref[
                s * PAIR : s * PAIR + CAP, 0 : 4 * HID
            ]
            out_ref[s * CAP : (s + 1) * CAP, 4 * HID : 6 * HID] = acc_ref[
                s * PAIR + CAP : (s + 1) * PAIR, 4 * HID : 6 * HID
            ]


def forward(core, xg, wg, wu, wd, wr):
    return pl.pallas_call(
        forward_kernel,
        grid=(NY,),
        in_specs=[scalar_spec(), pl.BlockSpec((1, ROWS, WIDTH), lambda i: (i, 0, 0))]
        + [weight_spec()] * 3
        + [pl.BlockSpec((3, HID, WIDTH), lambda i: (0, 0, i))],
        out_specs=whole((SLOTS, 6 * HID)),
        out_shape=jax.ShapeDtypeStruct((SLOTS, 6 * HID), F32),
        scratch_shapes=[pltpu.VMEM((ROWS, 6 * HID), F32)],
        name="forward",
    )(core, xg, wg, wu, wd, wr)


def backward_kernel(
    c_ref, own_ref, got_ref, wg_ref, wu_ref, wr_ref, out_ref, left_ref, grads_ref, spread_ref
):
    step = pl.program_id(0)

    @pl.when(step == 0)
    def _():
        def total(at):
            cols = slice(at * 2 * HID, (at + 1) * 2 * HID)
            return own_ref[:, cols] + pltpu.roll(got_ref[:, cols], HID, 1)

        pre_gate, pre_up, back = total(0), total(1), total(2)
        sig = 1.0 / (1.0 + jnp.exp(-pre_gate))
        silu = pre_gate * sig
        hidden = (silu * pre_up).astype(BF16).astype(F32)
        grad_gate = back * pre_up * sig * (1.0 + pre_gate * (1.0 - sig))
        grad_up = back * silu
        both = jnp.concatenate([grad_gate, grad_up], axis=1)
        grads_ref[...] = both.astype(BF16)
        gate = jnp.sum(hidden * back, axis=1, keepdims=True)
        row = iota((SLOTS, WIDTH), 0)
        lane = iota((SLOTS, WIDTH), 1)
        src = (row * 5462) >> 16
        want = (src >> 4) * TOK + row - src * CAP
        table = jnp.where(lane == want, jnp.broadcast_to(gate, (SLOTS, WIDTH)), 0.0)
        col = iota((16, SLOTS), 1)
        picks = jnp.where(((col * 5462) >> 16) % 16 == iota((16, SLOTS), 0), 1.0, 0.0)
        packed = jnp.dot(picks.astype(BF16), table.astype(BF16), preferred_element_type=F32)
        for y in range(NY):
            out_ref[y, SLOTS:BACK, :] = packed.astype(BF16)
        spread_ref[...] = jnp.zeros((ROWS, 6 * HID), F32)
        for s in range(EXPERTS):
            spread_ref[s * PAIR : s * PAIR + CAP, 0 : 4 * HID] = both[s * CAP : (s + 1) * CAP, :]
            spread_ref[s * PAIR + CAP : (s + 1) * PAIR, 4 * HID : 6 * HID] = hidden[
                s * CAP : (s + 1) * CAP, :
            ]
        flipped = spread_ref[...].T.astype(BF16)
        for at in range(3):
            left_ref[0, at * HID : (at + 1) * HID, :] = flipped[2 * at * HID : (2 * at + 1) * HID]
            left_ref[1, at * HID : (at + 1) * HID, :] = flipped[
                (2 * at + 1) * HID : (2 * at + 2) * HID
            ]

    off = pl.multiple_of(c_ref[0] * WIDTH, WIDTH)
    mats = jnp.concatenate(
        [wg_ref[:, pl.ds(off, WIDTH)], wr_ref[0], wu_ref[:, pl.ds(off, WIDTH)], wr_ref[1]], axis=0
    )
    rows = jnp.dot(grads_ref[...], mats, preferred_element_type=F32)
    out_ref[step, 0:SLOTS, :] = rows.astype(BF16)


def backward(core, own, got, wg, wu, wr):
    return pl.pallas_call(
        backward_kernel,
        grid=(NY,),
        in_specs=[scalar_spec(), whole((SLOTS, 6 * HID)), whole((SLOTS, 6 * HID))]
        + [weight_spec()] * 2
        + [pl.BlockSpec((2, HID, WIDTH), lambda i: (0, 0, i))],
        out_specs=(whole((NY, BACK, WIDTH)), whole((2, 3 * HID, ROWS))),
        out_shape=(
            jax.ShapeDtypeStruct((NY, BACK, WIDTH), BF16),
            jax.ShapeDtypeStruct((2, 3 * HID, ROWS), BF16),
        ),
        scratch_shapes=[pltpu.VMEM((SLOTS, 4 * HID), BF16), pltpu.VMEM((ROWS, 6 * HID), F32)],
        name="backward",
    )(core, own, got, wg, wu, wr)


def partner_kernel(left_ref, xg_ref, out_ref):
    out_ref[...] = jnp.dot(left_ref[0], xg_ref[0], preferred_element_type=F32).astype(BF16)


def partner_grads(left, xg):
    return pl.pallas_call(
        partner_kernel,
        grid=(NY,),
        in_specs=[
            pl.BlockSpec((1, 3 * HID, ROWS), lambda i: (1, 0, 0)),
            pl.BlockSpec((1, ROWS, WIDTH), lambda i: (i, 0, 0)),
        ],
        out_specs=pl.BlockSpec((3 * HID, WIDTH), lambda i: (0, i)),
        out_shape=jax.ShapeDtypeStruct((3 * HID, HALF), BF16),
        name="partner_grads",
    )(left, xg)


def merge_kernel(c_ref, left_ref, xg_ref, got_ref, gate_ref, up_ref, down_ref):
    off = pl.multiple_of(c_ref[0] * WIDTH, WIDTH)
    away = pl.multiple_of((1 - c_ref[0]) * WIDTH, WIDTH)
    mine = jnp.dot(left_ref[0], xg_ref[0], preferred_element_type=F32)
    for at, ref in enumerate((gate_ref, up_ref, down_ref)):
        ref[:, pl.ds(off, WIDTH)] = mine[at * HID : (at + 1) * HID, :]
        ref[:, pl.ds(away, WIDTH)] = got_ref[at * HID : (at + 1) * HID, :].astype(F32)


def merged_grads(core, left, xg, got):
    return pl.pallas_call(
        merge_kernel,
        grid=(NY,),
        in_specs=[
            scalar_spec(),
            pl.BlockSpec((1, 3 * HID, ROWS), lambda i: (0, 0, 0)),
            pl.BlockSpec((1, ROWS, WIDTH), lambda i: (i, 0, 0)),
            pl.BlockSpec((3 * HID, WIDTH), lambda i: (0, i)),
        ],
        out_specs=[pl.BlockSpec((HID, 2 * WIDTH), lambda i: (0, i))] * 3,
        out_shape=[jax.ShapeDtypeStruct((HID, 2 * HALF), F32)] * 3,
        name="merged_grads",
    )(core, left, xg, got)


def reduce_kernel(got_ref, out_ref, acc_ref):
    total = got_ref[0].astype(F32)
    for y in range(1, NY):
        total = total + got_ref[y].astype(F32)
    acc_ref[...] = total
    out_ref[...] = jnp.zeros((EXPERTS, 16, WIDTH), BF16)
    for s in range(EXPERTS):
        out_ref[s, 0:CAP, :] = acc_ref[s * CAP : (s + 1) * CAP, :].astype(BF16)
        lanes = slice((s // 16) * TOK, (s // 16 + 1) * TOK)
        out_ref[s, CAP : CAP + 1, 0:TOK] = acc_ref[
            SLOTS + s % 16 : SLOTS + s % 16 + 1, lanes
        ].astype(BF16)


def reduced(got):
    return pl.pallas_call(
        reduce_kernel,
        out_shape=jax.ShapeDtypeStruct((EXPERTS, 16, WIDTH), BF16),
        scratch_shapes=[pltpu.VMEM((BACK, WIDTH), F32)],
        name="reduced",
    )(got)


def combine_kernel(rt_ref, gw_ref, back_ref, out_ref, gate_ref):
    code, first, second = slot_codes(rt_ref[...])
    shape = (EXPERTS, 16, TOK)
    code3 = jnp.broadcast_to(code[:, None, :], shape)
    select = jnp.where(code3 == iota(shape, 1).astype(F32), 1.0, 0.0)
    select = select.reshape(EXPERTS * 16, TOK).T.astype(BF16)
    back = back_ref[...]
    rows = jnp.dot(
        select, back.reshape(EXPERTS * 16, WIDTH), preferred_element_type=F32
    )
    out_ref[...] = rows.astype(BF16)
    shares = back[:, CAP, 0:TOK].astype(F32)
    mine = jnp.zeros((EXPERTS, TOK), F32)
    for p in range(CAP):
        mine = mine + jnp.where(code == float(p), shares[:, p : p + 1], 0.0)
    top = jnp.sum(jnp.where(first, mine, 0.0), axis=0, keepdims=True)
    low = jnp.sum(jnp.where(second, mine, 0.0), axis=0, keepdims=True)
    gate_ref[...] = jnp.concatenate([top, low], axis=0) / gw_ref[...]


def combine(rt, gw, back):
    return pl.pallas_call(
        combine_kernel,
        out_shape=(
            jax.ShapeDtypeStruct((TOK, WIDTH), BF16),
            jax.ShapeDtypeStruct((TOP, TOK), F32),
        ),
        name="combine",
    )(rt, gw, back)


def core_swap(value):
    return lax.ppermute(value, "c", [(0, 1), (1, 0)])


def shards(tokens, cotangent, routes, gate_weight, w_gate, w_up, w_down, shared_hidden):
    rt, gw = routes.T, gate_weight.T
    core = lax.axis_index("c").astype(I32).reshape(1)
    wg, wu, wd = w_gate[0], w_up[0], w_down[0]
    sent = dispatch(rt, gw, tokens, cotangent)
    rows = lax.all_to_all(sent, EP, split_axis=0, concat_axis=0, tiled=True)
    rows, cotangent, wg, wu, wd = lax.optimization_barrier((rows, cotangent, wg, wu, wd))
    xg = lax.all_gather(rows.reshape(ROWS, WIDTH), "y", axis=0, tiled=False)

    wr = core_swap(other_half(core, wg, wu, wd))
    shared = lax.dot_general(
        shared_hidden, cotangent, (((0,), (0,)), ((), ())), preferred_element_type=F32
    ).astype(BF16)
    shared = lax.all_to_all(
        shared.reshape(EXPERTS, -1, WIDTH), EP, split_axis=0, concat_axis=0, tiled=True
    )
    shared_grad = jnp.sum(shared.astype(F32), axis=0)
    xg, wr, shared_grad = lax.optimization_barrier((xg, wr, shared_grad))

    own = forward(core, xg, wg, wu, wd, wr)
    parts, left = backward(core, own, core_swap(own), wg, wu, wr)
    theirs = core_swap(partner_grads(left, xg))
    grads = merged_grads(core, left, xg, theirs)
    got = lax.all_to_all(parts, "y", split_axis=0, concat_axis=0, tiled=True)
    back = lax.all_to_all(reduced(got), EP, split_axis=0, concat_axis=0, tiled=True)
    tokens_grad, gate_grad = combine(rt, gw, back)
    return (tokens_grad, gate_grad.T, grads[0][None], grads[1][None], grads[2][None], shared_grad)


def solution(mesh):
    split = Mesh(mesh.devices.reshape(8, 4, 8, 2), ("z", "x", "y", "c"))
    ep, tp = ("z", "x"), ("y", "c")
    placed = (
        P(ep, tp),
        P(ep, tp),
        P(ep, None),
        P(ep, None),
        P(ep, tp, None),
        P(ep, tp, None),
        P(ep, tp, None),
        P(ep, None),
    )
    return jax.shard_map(
        shards,
        mesh=split,
        in_specs=placed,
        out_specs=(
            P(ep, tp),
            P(ep, None),
            P(ep, tp, None),
            P(ep, tp, None),
            P(ep, tp, None),
            P(ep, tp),
        ),
        check_vma=False,
    )
```

```python
import jax
import jax.numpy as jnp
from jax import lax
from jax.experimental import pallas as pl
from jax.experimental.pallas import tpu as pltpu
from jax.sharding import Mesh, PartitionSpec as P

TOK, TOP, EXPERTS, CAP = 128, 2, 32, 12
SLOTS = EXPERTS * CAP
ROWS = 2 * SLOTS
PAIR = 2 * CAP
WIDTH = 256
NY = 8
HALF = NY * WIDTH
HID = 64
EP = ("z", "x")
F32, BF16, I32 = jnp.float32, jnp.bfloat16, jnp.int32


def iota(shape, dim):
    return lax.broadcasted_iota(I32, shape, dim)


def slot_codes(rt):
    ids = iota((EXPERTS, TOK), 0)
    first, second = rt[0:1, :] == ids, rt[1:2, :] == ids
    hot = jnp.where(first, 1.0, 0.0) + jnp.where(second, 1.0, 0.0)
    upper = jnp.where(iota((TOK, TOK), 0) < iota((TOK, TOK), 1), 1.0, 0.0)
    rank = jnp.dot(hot.astype(BF16), upper.astype(BF16), preferred_element_type=F32)
    return jnp.where(hot > 0.5, rank, -1.0), first, second


def dispatch_kernel(rt_ref, gw_ref, tok_ref, cot_ref, out_ref):
    code, first, second = slot_codes(rt_ref[...])
    gw = gw_ref[...]
    weight = jnp.where(first, gw[0:1, :], 0.0) + jnp.where(second, gw[1:2, :], 0.0)
    shape = (EXPERTS, PAIR, TOK)
    code3 = jnp.broadcast_to(code[:, None, :], shape)
    weight3 = jnp.broadcast_to(weight[:, None, :], shape)
    at = iota(shape, 1)
    atf = at.astype(F32)
    sel_x = jnp.where(code3 == atf, jnp.where(at < CAP, 1.0, 0.0), 0.0)
    sel_g = jnp.where(code3 == atf - float(CAP), jnp.where(at >= CAP, 1.0, 0.0), 0.0)
    scale = jnp.sum(sel_g * weight3 + sel_x, axis=2, keepdims=True).reshape(ROWS, 1)
    select = jnp.concatenate(
        [sel_x.reshape(ROWS, TOK).astype(BF16), sel_g.reshape(ROWS, TOK).astype(BF16)], axis=1
    )
    source = jnp.concatenate([tok_ref[...], cot_ref[...]], axis=0)
    rows = jnp.dot(select, source, preferred_element_type=F32)
    out_ref[...] = (rows * scale).astype(BF16).reshape(EXPERTS, PAIR, WIDTH)


def dispatch(rt, gw, tokens, cotangent):
    out = (jax.ShapeDtypeStruct((EXPERTS, PAIR, WIDTH), BF16),)
    return kernel_call(dispatch_kernel, out, "dispatch", rt, gw, tokens, cotangent)[0]


def vmem(value):
    return pltpu.with_memory_space_constraint(value, pltpu.VMEM)


def kernel_call(body, out, name, *values, core=None, scratch=(), far=(), near=(), far_out=0):
    specs = [pl.BlockSpec(memory_space=pl.ANY)] * len(far)
    specs += [pl.BlockSpec(memory_space=pltpu.VMEM)] * len(near)
    specs += [pl.BlockSpec()] * len(values)
    values = [*far, *(vmem(v) for v in near), *values]
    if core is not None:
        specs, values = [pl.BlockSpec(memory_space=pltpu.SMEM)] + specs, [core] + values
    results = [
        pl.BlockSpec(memory_space=pl.ANY) if at < far_out else pl.BlockSpec()
        for at in range(len(out))
    ]
    return pl.pallas_call(
        body,
        in_specs=specs,
        out_specs=results,
        out_shape=list(out),
        scratch_shapes=list(scratch),
        name=name,
    )(*values)


def fetch(pairs, sems):
    copies = [
        pltpu.make_async_copy(there, here, sems.at[at]) for at, (there, here) in enumerate(pairs)
    ]
    for copy in copies:
        copy.start()
    return copies


def flags(count):
    return pltpu.SemaphoreType.DMA((count,))


def lanes_of(step, half):
    return pl.ds(pl.multiple_of((2 * step + half) * WIDTH, WIDTH), WIDTH)


def half_lanes(y):
    return slice(y * WIDTH, (y + 1) * WIDTH)


def split_kernel(c_ref, wg_ref, wu_ref, wd_ref, out_ref):
    for at, ref in enumerate((wg_ref, wu_ref, wd_ref)):
        for y in range(NY):
            out_ref[at, :, half_lanes(y)] = ref[:, lanes_of(y, 1 - c_ref[0])]


def other_half(core, wg, wu, wd):
    out = (jax.ShapeDtypeStruct((3, HID, HALF), BF16),)
    return kernel_call(split_kernel, out, "other_half", wg, wu, wd, core=core)[0]


def is_token_lane(shape):
    lane = iota(shape, 1)
    return lane - ((lane * 2731) >> 16) * PAIR < CAP


def forward_kernel(
    c_ref, xg_far, wg_far, wu_far, wd_far, wr_far, out_ref, xg_ref, wg_ref, wu_ref, wd_ref, wr_ref, sems
):
    weights = [(wg_far, wg_ref), (wd_far, wd_ref), (wu_far, wu_ref), (wr_far, wr_ref)]
    blocks = [(xg_far.at[y], xg_ref.at[y]) for y in range(NY)]
    copies = fetch(blocks[:1] + weights + blocks[1:], sems)
    for copy in copies[:5]:
        copy.wait()
    total = None
    for y in range(NY):
        if y > 0:
            copies[4 + y].wait()
        parts = []
        for at, ref in enumerate((wg_ref, wd_ref, wu_ref)):
            parts.append(ref[:, lanes_of(y, c_ref[0])])
            parts.append(wr_ref[(0, 2, 1)[at], :, half_lanes(y)])
        part = lax.dot_general(
            jnp.concatenate(parts, axis=0),
            xg_ref[y],
            (((1,), (1,)), ((), ())),
            preferred_element_type=F32,
        )
        total = part if total is None else total + part
    pair = 2 * HID
    out_ref[0:pair, :] = jnp.where(
        is_token_lane((pair, ROWS)), total[0:pair, :], total[pair : 2 * pair, :]
    )
    out_ref[pair : 2 * pair, :] = total[2 * pair : 3 * pair, :]


def forward(core, xg, wg, wu, wd, wr):
    out = (jax.ShapeDtypeStruct((4 * HID, ROWS), F32),)
    return kernel_call(
        forward_kernel,
        out,
        "forward",
        core=core,
        far=(xg, wg, wu, wd, wr),
        scratch=(
            pltpu.VMEM((NY, ROWS, WIDTH), BF16),
            pltpu.VMEM((HID, 2 * HALF), BF16),
            pltpu.VMEM((HID, 2 * HALF), BF16),
            pltpu.VMEM((HID, 2 * HALF), BF16),
            pltpu.VMEM((3, HID, HALF), BF16),
            flags(4 + NY),
        ),
    )[0]


def backward_kernel(
    c_ref, own_far, wg_far, wu_far, wr_far, got_ref, out_far, gate_ref, left_ref,
    own_ref, wg_ref, wu_ref, wr_ref, out_ref, sems, out_sems,
):
    copies = fetch(
        [
            (own_far, own_ref),
            (wg_far, wg_ref),
            (wu_far, wu_ref),
            (wr_far.at[0:2], wr_ref),
        ],
        sems,
    )
    copies[0].wait()

    def total(at):
        low, mid, high = 2 * at * HID, (2 * at + 1) * HID, (2 * at + 2) * HID
        return jnp.concatenate(
            [
                own_ref[low:mid, :] + got_ref[mid:high, :],
                own_ref[mid:high, :] + got_ref[low:mid, :],
            ],
            axis=0,
        )

    pre_gate, pre_up = total(0), total(1)
    keep = is_token_lane((2 * HID, ROWS))
    back = pltpu.roll(pre_gate, ROWS - CAP, 1)
    sig = 1.0 / (1.0 + jnp.exp(-jnp.where(keep, pre_gate, 0.0)))
    silu = pre_gate * sig
    hidden = jnp.where(keep, silu * pre_up, 0.0).astype(BF16).astype(F32)
    grad_gate = jnp.where(keep, back * pre_up * sig * (1.0 + pre_gate * (1.0 - sig)), 0.0)
    grad_up = jnp.where(keep, back * silu, 0.0)
    gate_ref[...] = jnp.broadcast_to(
        jnp.sum(hidden * back, axis=0, keepdims=True)[None], (NY, 1, ROWS)
    )
    shifted = pltpu.roll(hidden, CAP, 1)
    for at, grad in enumerate((grad_gate, grad_up, shifted)):
        grad = grad.astype(BF16)
        left_ref[0, at * HID : (at + 1) * HID, :] = grad[0:HID]
        left_ref[1, at * HID : (at + 1) * HID, :] = grad[HID : 2 * HID]
    both = jnp.concatenate([grad_gate.astype(BF16), grad_up.astype(BF16)], axis=0)
    slot = iota((SLOTS, ROWS), 0)
    lane = iota((SLOTS, ROWS), 1)
    compact = jnp.where(lane == slot + ((slot * 5462) >> 16) * CAP, 1.0, 0.0).astype(BF16)
    grads = lax.dot_general(
        compact, both, (((1,), (1,)), ((), ())), preferred_element_type=F32
    ).astype(BF16)
    for copy in copies[1:]:
        copy.wait()
    sent = []
    for y in range(NY):
        mats = jnp.concatenate(
            [
                wg_ref[:, lanes_of(y, c_ref[0])],
                wr_ref[0, :, half_lanes(y)],
                wu_ref[:, lanes_of(y, c_ref[0])],
                wr_ref[1, :, half_lanes(y)],
            ],
            axis=0,
        )
        out_ref[y] = jnp.dot(grads, mats, preferred_element_type=F32).astype(BF16)
        sent.append(pltpu.make_async_copy(out_ref.at[y], out_far.at[y], out_sems.at[y]))
        sent[y].start()
    for copy in sent:
        copy.wait()


def backward(core, own, got, wg, wu, wr):
    out = (
        jax.ShapeDtypeStruct((NY, SLOTS, WIDTH), BF16),
        jax.ShapeDtypeStruct((NY, 1, ROWS), F32),
        jax.ShapeDtypeStruct((2, 3 * HID, ROWS), BF16),
    )
    return kernel_call(
        backward_kernel,
        out,
        "backward",
        core=core,
        far=(own, wg, wu, wr),
        near=(got,),
        far_out=1,
        scratch=(
            pltpu.VMEM((4 * HID, ROWS), F32),
            pltpu.VMEM((HID, 2 * HALF), BF16),
            pltpu.VMEM((HID, 2 * HALF), BF16),
            pltpu.VMEM((2, HID, HALF), BF16),
            pltpu.VMEM((NY, SLOTS, WIDTH), BF16),
            flags(4),
            flags(NY),
        ),
    )


def partner_kernel(left_far, xg_far, out_ref, left_ref, xg_ref, sems):
    copies = fetch(
        [(left_far.at[1], left_ref)] + [(xg_far.at[y], xg_ref.at[y]) for y in range(NY)], sems
    )
    copies[0].wait()
    for y in range(NY):
        copies[1 + y].wait()
        out_ref[:, half_lanes(y)] = jnp.dot(
            left_ref[...], xg_ref[y], preferred_element_type=F32
        ).astype(BF16)


def partner_grads(left, xg):
    return kernel_call(
        partner_kernel,
        (jax.ShapeDtypeStruct((3 * HID, HALF), BF16),),
        "partner_grads",
        far=(left, xg),
        scratch=(
            pltpu.VMEM((3 * HID, ROWS), BF16),
            pltpu.VMEM((NY, ROWS, WIDTH), BF16),
            flags(1 + NY),
        ),
    )[0]


def merge_kernel(
    c_ref, left_far, xg_far, got_far, gate_far, up_far, down_far, left_ref, xg_ref, got_ref, out_ref, sems, out_sems
):
    copies = fetch(
        [(left_far.at[0], left_ref), (got_far, got_ref)]
        + [(xg_far.at[y], xg_ref.at[y]) for y in range(NY)],
        sems,
    )
    copies[0].wait()
    copies[1].wait()
    sent = []
    for y in range(NY):
        copies[2 + y].wait()
        mine = jnp.dot(left_ref[...], xg_ref[y], preferred_element_type=F32)
        theirs = got_ref[:, half_lanes(y)].astype(F32)
        both = slice(2 * y * WIDTH, (2 * y + 2) * WIDTH)
        for at, far in enumerate((gate_far, up_far, down_far)):
            rows = slice(at * HID, (at + 1) * HID)
            out_ref[at, :, lanes_of(y, c_ref[0])] = mine[rows, :]
            out_ref[at, :, lanes_of(y, 1 - c_ref[0])] = theirs[rows, :]
            sent.append(
                pltpu.make_async_copy(
                    out_ref.at[at, :, both], far.at[:, both], out_sems.at[3 * y + at]
                )
            )
            sent[-1].start()
    for copy in sent:
        copy.wait()


def merged_grads(core, left, xg, got):
    return kernel_call(
        merge_kernel,
        [jax.ShapeDtypeStruct((HID, 2 * HALF), F32)] * 3,
        "merged_grads",
        core=core,
        far=(left, xg, got),
        far_out=3,
        scratch=(
            pltpu.VMEM((3 * HID, ROWS), BF16),
            pltpu.VMEM((NY, ROWS, WIDTH), BF16),
            pltpu.VMEM((3 * HID, HALF), BF16),
            pltpu.VMEM((3, HID, 2 * HALF), F32),
            flags(2 + NY),
            flags(3 * NY),
        ),
    )


def reduce_kernel(got_ref, gate_ref, out_ref):
    total = got_ref[0].astype(F32)
    gate = gate_ref[0]
    for y in range(1, NY):
        total = total + got_ref[y].astype(F32)
        gate = gate + gate_ref[y]
    total = total.astype(BF16)
    src = iota((EXPERTS, ROWS), 0)
    lane = iota((EXPERTS, ROWS), 1)
    table = jnp.where(
        (lane * 2731) >> 16 == src, jnp.broadcast_to(gate, (EXPERTS, ROWS)), 0.0
    ).astype(BF16)
    at = iota((ROWS, WIDTH), 0)
    picks = jnp.where(
        at - ((at * 2731) >> 16) * PAIR == iota((ROWS, WIDTH), 1), 1.0, 0.0
    ).astype(BF16)
    shares = jnp.dot(table, picks, preferred_element_type=F32).astype(BF16)
    row = iota((EXPERTS * 16, SLOTS + EXPERTS), 0)
    col = iota((EXPERTS * 16, SLOTS + EXPERTS), 1)
    source = row >> 4
    want = jnp.where(
        row - source * 16 < CAP,
        source * CAP + row - source * 16,
        jnp.where(row - source * 16 == CAP, SLOTS + source, -1),
    )
    place = jnp.where(col == want, 1.0, 0.0).astype(BF16)
    rows = jnp.dot(
        place, jnp.concatenate([total, shares], axis=0), preferred_element_type=F32
    )
    out_ref[...] = rows.astype(BF16).reshape(EXPERTS, 16, WIDTH)


def reduced(got, gate):
    return kernel_call(
        reduce_kernel,
        (jax.ShapeDtypeStruct((EXPERTS, 16, WIDTH), BF16),),
        "reduced",
        gate,
        near=(got,),
    )[0]


def combine_kernel(back_ref, rt_ref, gw_ref, out_ref, gate_ref):
    code, first, second = slot_codes(rt_ref[...])
    shape = (EXPERTS, 16, TOK)
    code3 = jnp.broadcast_to(code[:, None, :], shape)
    select = jnp.where(code3 == iota(shape, 1).astype(F32), 1.0, 0.0)
    select = select.reshape(EXPERTS * 16, TOK).T.astype(BF16)
    back = back_ref[...]
    rows = jnp.dot(
        select, back.reshape(EXPERTS * 16, WIDTH), preferred_element_type=F32
    )
    out_ref[...] = rows.astype(BF16)
    shares = back[:, CAP, 0:TOK].astype(F32)
    mine = jnp.zeros((EXPERTS, TOK), F32)
    for p in range(CAP):
        mine = mine + jnp.where(code == float(p), shares[:, p : p + 1], 0.0)
    top = jnp.sum(jnp.where(first, mine, 0.0), axis=0, keepdims=True)
    low = jnp.sum(jnp.where(second, mine, 0.0), axis=0, keepdims=True)
    gate_ref[...] = jnp.concatenate([top, low], axis=0) / gw_ref[...]


def combine(rt, gw, back):
    out = (
        jax.ShapeDtypeStruct((TOK, WIDTH), BF16),
        jax.ShapeDtypeStruct((TOP, TOK), F32),
    )
    return kernel_call(combine_kernel, out, "combine", rt, gw, near=(back,))


def core_swap(value):
    return lax.ppermute(value, "c", [(0, 1), (1, 0)])


def shards(tokens, cotangent, routes, gate_weight, w_gate, w_up, w_down, shared_hidden):
    rt, gw = routes.T, gate_weight.T
    core = lax.axis_index("c").astype(I32).reshape(1)
    wg, wu, wd = w_gate[0], w_up[0], w_down[0]
    sent = dispatch(rt, gw, tokens, cotangent)
    rows = lax.all_to_all(sent, EP, split_axis=0, concat_axis=0, tiled=True)
    rows, cotangent, wg, wu, wd = lax.optimization_barrier((rows, cotangent, wg, wu, wd))
    xg = lax.all_gather(rows.reshape(ROWS, WIDTH), "y", axis=0, tiled=False)

    wr = core_swap(other_half(core, wg, wu, wd))
    shared = lax.dot_general(
        shared_hidden, cotangent, (((0,), (0,)), ((), ())), preferred_element_type=F32
    ).astype(BF16)
    shared = lax.all_to_all(
        shared.reshape(EXPERTS, -1, WIDTH), EP, split_axis=0, concat_axis=0, tiled=True
    )
    shared_grad = jnp.sum(shared.astype(F32), axis=0)
    xg, wr, shared_grad = lax.optimization_barrier((xg, wr, shared_grad))

    own = forward(core, xg, wg, wu, wd, wr)
    parts, gate, left = backward(core, own, core_swap(own), wg, wu, wr)
    got = lax.all_to_all(parts, "y", split_axis=0, concat_axis=0, tiled=True)
    theirs = partner_grads(left, xg)
    theirs, gate = lax.optimization_barrier((theirs, gate))
    theirs = core_swap(theirs)
    gate = lax.all_to_all(gate, "y", split_axis=0, concat_axis=0, tiled=True)
    grads = merged_grads(core, left, xg, theirs)
    back = lax.all_to_all(reduced(got, gate), EP, split_axis=0, concat_axis=0, tiled=True)
    tokens_grad, gate_grad = combine(rt, gw, back)
    return (tokens_grad, gate_grad.T, grads[0][None], grads[1][None], grads[2][None], shared_grad)


def solution(mesh):
    split = Mesh(mesh.devices.reshape(8, 4, 8, 2), ("z", "x", "y", "c"))
    ep, tp = ("z", "x"), ("y", "c")
    placed = (
        P(ep, tp),
        P(ep, tp),
        P(ep, None),
        P(ep, None),
        P(ep, tp, None),
        P(ep, tp, None),
        P(ep, tp, None),
        P(ep, None),
    )
    return jax.shard_map(
        shards,
        mesh=split,
        in_specs=placed,
        out_specs=(
            P(ep, tp),
            P(ep, None),
            P(ep, tp, None),
            P(ep, tp, None),
            P(ep, tp, None),
            P(ep, tp),
        ),
        check_vma=False,
    )
```

```python
import jax
import jax.numpy as jnp
from jax import lax
from jax.experimental import pallas as pl
from jax.experimental.pallas import tpu as pltpu
from jax.sharding import Mesh, PartitionSpec as P

TOK, TOP, EXPERTS, CAP = 128, 2, 32, 12
SLOTS = EXPERTS * CAP
ROWS = 2 * SLOTS
PAIR = 2 * CAP
WIDTH = 256
NY = 8
HALF = NY * WIDTH
HID = 64
BACK = SLOTS + 8
EP = ("z", "x")
F32, BF16, I32 = jnp.float32, jnp.bfloat16, jnp.int32


def iota(shape, dim):
    return lax.broadcasted_iota(I32, shape, dim)


def slot_codes(rt):
    ids = iota((EXPERTS, TOK), 0)
    first, second = rt[0:1, :] == ids, rt[1:2, :] == ids
    hot = jnp.where(first, 1.0, 0.0) + jnp.where(second, 1.0, 0.0)
    upper = jnp.where(iota((TOK, TOK), 0) < iota((TOK, TOK), 1), 1.0, 0.0)
    rank = jnp.dot(hot.astype(BF16), upper.astype(BF16), preferred_element_type=F32)
    return jnp.where(hot > 0.5, rank, -1.0), first, second


def dispatch_kernel(rt_ref, gw_ref, tok_ref, cot_ref, out_ref):
    code, first, second = slot_codes(rt_ref[...])
    gw = gw_ref[...]
    weight = jnp.where(first, gw[0:1, :], 0.0) + jnp.where(second, gw[1:2, :], 0.0)
    shape = (EXPERTS, PAIR, TOK)
    code3 = jnp.broadcast_to(code[:, None, :], shape)
    weight3 = jnp.broadcast_to(weight[:, None, :], shape)
    at = iota(shape, 1)
    atf = at.astype(F32)
    sel_x = jnp.where(code3 == atf, jnp.where(at < CAP, 1.0, 0.0), 0.0)
    sel_g = jnp.where(code3 == atf - float(CAP), jnp.where(at >= CAP, 1.0, 0.0), 0.0)
    scale = jnp.sum(sel_g * weight3 + sel_x, axis=2, keepdims=True).reshape(ROWS, 1)
    select = jnp.concatenate(
        [sel_x.reshape(ROWS, TOK).astype(BF16), sel_g.reshape(ROWS, TOK).astype(BF16)], axis=1
    )
    source = jnp.concatenate([tok_ref[...], cot_ref[...]], axis=0)
    rows = jnp.dot(select, source, preferred_element_type=F32)
    out_ref[...] = (rows * scale).astype(BF16).reshape(EXPERTS, PAIR, WIDTH)


def dispatch(rt, gw, tokens, cotangent):
    out = (pltpu.VMEM((EXPERTS, PAIR, WIDTH), BF16),)
    return kernel_call(dispatch_kernel, out, "dispatch", rt, gw, tokens, cotangent)[0]


def vmem(value):
    return pltpu.with_memory_space_constraint(value, pltpu.VMEM)


def kernel_call(body, out, name, *values, core=None, scratch=(), far=(), near=(), far_out=0):
    specs = [pl.BlockSpec(memory_space=pl.ANY)] * len(far)
    specs += [pl.BlockSpec(memory_space=pltpu.VMEM)] * len(near)
    specs += [pl.BlockSpec()] * len(values)
    values = [*far, *(vmem(v) for v in near), *values]
    if core is not None:
        specs, values = [pl.BlockSpec(memory_space=pltpu.SMEM)] + specs, [core] + values
    results = [
        pl.BlockSpec(memory_space=pl.ANY)
        if at < far_out
        else pl.BlockSpec()
        if isinstance(shape, jax.ShapeDtypeStruct)
        else pl.BlockSpec(memory_space=pltpu.VMEM)
        for at, shape in enumerate(out)
    ]
    return pl.pallas_call(
        body,
        in_specs=specs,
        out_specs=results,
        out_shape=list(out),
        scratch_shapes=list(scratch),
        name=name,
    )(*values)


def fetch(pairs, sems):
    copies = [
        pltpu.make_async_copy(there, here, sems.at[at]) for at, (there, here) in enumerate(pairs)
    ]
    for copy in copies:
        copy.start()
    return copies


def flags(count):
    return pltpu.SemaphoreType.DMA((count,))


def lanes_of(step, half):
    return pl.ds(pl.multiple_of((2 * step + half) * WIDTH, WIDTH), WIDTH)


def half_lanes(y):
    return slice(y * WIDTH, (y + 1) * WIDTH)


def split_kernel(c_ref, wg_ref, wu_ref, wd_ref, out_ref):
    for at, ref in enumerate((wg_ref, wu_ref, wd_ref)):
        for y in range(NY):
            out_ref[at, :, half_lanes(y)] = ref[:, lanes_of(y, 1 - c_ref[0])]


def other_half(core, wg, wu, wd):
    out = (jax.ShapeDtypeStruct((3, HID, HALF), BF16),)
    return kernel_call(split_kernel, out, "other_half", wg, wu, wd, core=core)[0]


def is_token_lane(shape):
    lane = iota(shape, 1)
    return lane - ((lane * 2731) >> 16) * PAIR < CAP


def forward_kernel(
    c_ref, xg_far, wg_far, wu_far, wd_far, wr_far, out_ref, xg_ref, wg_ref, wu_ref, wd_ref, wr_ref, sems
):
    weights = [(wg_far, wg_ref), (wd_far, wd_ref), (wu_far, wu_ref), (wr_far, wr_ref)]
    blocks = [(xg_far.at[y], xg_ref.at[y]) for y in range(NY)]
    copies = fetch(blocks[:1] + weights + blocks[1:], sems)
    for copy in copies[:5]:
        copy.wait()
    total = None
    for y in range(NY):
        if y > 0:
            copies[4 + y].wait()
        parts = []
        for at, ref in enumerate((wg_ref, wd_ref, wu_ref)):
            parts.append(ref[:, lanes_of(y, c_ref[0])])
            parts.append(wr_ref[(0, 2, 1)[at], :, half_lanes(y)])
        part = lax.dot_general(
            jnp.concatenate(parts, axis=0),
            xg_ref[y],
            (((1,), (1,)), ((), ())),
            preferred_element_type=F32,
        )
        total = part if total is None else total + part
    pair = 2 * HID
    out_ref[0:pair, :] = jnp.where(
        is_token_lane((pair, ROWS)), total[0:pair, :], total[pair : 2 * pair, :]
    )
    out_ref[pair : 2 * pair, :] = total[2 * pair : 3 * pair, :]


def forward(core, xg, wg, wu, wd, wr):
    out = (jax.ShapeDtypeStruct((4 * HID, ROWS), F32),)
    return kernel_call(
        forward_kernel,
        out,
        "forward",
        core=core,
        far=(xg, wg, wu, wd, wr),
        scratch=(
            pltpu.VMEM((NY, ROWS, WIDTH), BF16),
            pltpu.VMEM((HID, 2 * HALF), BF16),
            pltpu.VMEM((HID, 2 * HALF), BF16),
            pltpu.VMEM((HID, 2 * HALF), BF16),
            pltpu.VMEM((3, HID, HALF), BF16),
            flags(4 + NY),
        ),
    )[0]


def backward_kernel(
    c_ref, own_far, wg_far, wu_far, wr_far, got_ref, out_far, left_ref,
    own_ref, wg_ref, wu_ref, wr_ref, out_ref, sems, out_sems,
):
    copies = fetch(
        [
            (own_far, own_ref),
            (wg_far, wg_ref),
            (wu_far, wu_ref),
            (wr_far.at[0:2], wr_ref),
        ],
        sems,
    )
    copies[0].wait()

    def total(at):
        low, mid, high = 2 * at * HID, (2 * at + 1) * HID, (2 * at + 2) * HID
        return jnp.concatenate(
            [
                own_ref[low:mid, :] + got_ref[mid:high, :],
                own_ref[mid:high, :] + got_ref[low:mid, :],
            ],
            axis=0,
        )

    pre_gate, pre_up = total(0), total(1)
    keep = is_token_lane((2 * HID, ROWS))
    back = pltpu.roll(pre_gate, ROWS - CAP, 1)
    sig = 1.0 / (1.0 + jnp.exp(-jnp.where(keep, pre_gate, 0.0)))
    silu = pre_gate * sig
    hidden = jnp.where(keep, silu * pre_up, 0.0).astype(BF16).astype(F32)
    grad_gate = jnp.where(keep, back * pre_up * sig * (1.0 + pre_gate * (1.0 - sig)), 0.0)
    grad_up = jnp.where(keep, back * silu, 0.0)
    gate = jnp.sum(hidden * back, axis=0, keepdims=True)
    upper = gate.astype(BF16).astype(F32)
    tail = [part[:, half_lanes(at)] for part in (upper, gate - upper) for at in range(3)]
    tail = jnp.concatenate(tail + [jnp.zeros((2, WIDTH), F32)], axis=0).astype(BF16)
    shifted = pltpu.roll(hidden, CAP, 1)
    for at, grad in enumerate((grad_gate, grad_up, shifted)):
        grad = grad.astype(BF16)
        left_ref[0, at * HID : (at + 1) * HID, :] = grad[0:HID]
        left_ref[1, at * HID : (at + 1) * HID, :] = grad[HID : 2 * HID]
    both = jnp.concatenate([grad_gate.astype(BF16), grad_up.astype(BF16)], axis=0)
    slot = iota((SLOTS, ROWS), 0)
    lane = iota((SLOTS, ROWS), 1)
    compact = jnp.where(lane == slot + ((slot * 5462) >> 16) * CAP, 1.0, 0.0).astype(BF16)
    grads = lax.dot_general(
        compact, both, (((1,), (1,)), ((), ())), preferred_element_type=F32
    ).astype(BF16)
    for copy in copies[1:]:
        copy.wait()
    sent = []
    for y in range(NY):
        mats = jnp.concatenate(
            [
                wg_ref[:, lanes_of(y, c_ref[0])],
                wr_ref[0, :, half_lanes(y)],
                wu_ref[:, lanes_of(y, c_ref[0])],
                wr_ref[1, :, half_lanes(y)],
            ],
            axis=0,
        )
        out_ref[y, 0:SLOTS, :] = jnp.dot(grads, mats, preferred_element_type=F32).astype(BF16)
        out_ref[y, SLOTS:BACK, :] = tail
        sent.append(pltpu.make_async_copy(out_ref.at[y], out_far.at[y], out_sems.at[y]))
        sent[y].start()
    for copy in sent:
        copy.wait()


def backward(core, own, got, wg, wu, wr):
    out = (
        jax.ShapeDtypeStruct((NY, BACK, WIDTH), BF16),
        jax.ShapeDtypeStruct((2, 3 * HID, ROWS), BF16),
    )
    return kernel_call(
        backward_kernel,
        out,
        "backward",
        core=core,
        far=(own, wg, wu, wr),
        near=(got,),
        far_out=1,
        scratch=(
            pltpu.VMEM((4 * HID, ROWS), F32),
            pltpu.VMEM((HID, 2 * HALF), BF16),
            pltpu.VMEM((HID, 2 * HALF), BF16),
            pltpu.VMEM((2, HID, HALF), BF16),
            pltpu.VMEM((NY, BACK, WIDTH), BF16),
            flags(4),
            flags(NY),
        ),
    )


def partner_kernel(left_far, xg_far, out_ref, left_ref, xg_ref, sems):
    copies = fetch(
        [(left_far.at[1], left_ref)] + [(xg_far.at[y], xg_ref.at[y]) for y in range(NY)], sems
    )
    copies[0].wait()
    for y in range(NY):
        copies[1 + y].wait()
        out_ref[:, half_lanes(y)] = jnp.dot(
            left_ref[...], xg_ref[y], preferred_element_type=F32
        ).astype(BF16)


def partner_grads(left, xg):
    return kernel_call(
        partner_kernel,
        (jax.ShapeDtypeStruct((3 * HID, HALF), BF16),),
        "partner_grads",
        far=(left, xg),
        scratch=(
            pltpu.VMEM((3 * HID, ROWS), BF16),
            pltpu.VMEM((NY, ROWS, WIDTH), BF16),
            flags(1 + NY),
        ),
    )[0]


def merge_kernel(
    c_ref, left_far, xg_far, got_far, gate_far, up_far, down_far, left_ref, xg_ref, got_ref, out_ref, sems, out_sems
):
    copies = fetch(
        [(left_far.at[0], left_ref), (got_far, got_ref)]
        + [(xg_far.at[y], xg_ref.at[y]) for y in range(NY)],
        sems,
    )
    copies[0].wait()
    copies[1].wait()
    sent = []
    for y in range(NY):
        copies[2 + y].wait()
        mine = jnp.dot(left_ref[...], xg_ref[y], preferred_element_type=F32)
        theirs = got_ref[:, half_lanes(y)].astype(F32)
        both = slice(2 * y * WIDTH, (2 * y + 2) * WIDTH)
        for at, far in enumerate((gate_far, up_far, down_far)):
            rows = slice(at * HID, (at + 1) * HID)
            out_ref[at, :, lanes_of(y, c_ref[0])] = mine[rows, :]
            out_ref[at, :, lanes_of(y, 1 - c_ref[0])] = theirs[rows, :]
            sent.append(
                pltpu.make_async_copy(
                    out_ref.at[at, :, both], far.at[:, both], out_sems.at[3 * y + at]
                )
            )
            sent[-1].start()
    for copy in sent:
        copy.wait()


def merged_grads(core, left, xg, got):
    return kernel_call(
        merge_kernel,
        [jax.ShapeDtypeStruct((HID, 2 * HALF), F32)] * 3,
        "merged_grads",
        core=core,
        far=(left, xg, got),
        far_out=3,
        scratch=(
            pltpu.VMEM((3 * HID, ROWS), BF16),
            pltpu.VMEM((NY, ROWS, WIDTH), BF16),
            pltpu.VMEM((3 * HID, HALF), BF16),
            pltpu.VMEM((3, HID, 2 * HALF), F32),
            flags(2 + NY),
            flags(3 * NY),
        ),
    )


def place_kernel(got_ref, out_ref):
    total = got_ref[...].astype(F32)
    gate = total[SLOTS : SLOTS + 3, :] + total[SLOTS + 3 : SLOTS + 6, :]
    gate = jnp.concatenate([gate[at : at + 1, :] for at in range(3)], axis=1)
    total = total[0:SLOTS, :].astype(BF16)
    src = iota((EXPERTS, ROWS), 0)
    lane = iota((EXPERTS, ROWS), 1)
    table = jnp.where(
        (lane * 2731) >> 16 == src, jnp.broadcast_to(gate, (EXPERTS, ROWS)), 0.0
    ).astype(BF16)
    at = iota((ROWS, WIDTH), 0)
    picks = jnp.where(
        at - ((at * 2731) >> 16) * PAIR == iota((ROWS, WIDTH), 1), 1.0, 0.0
    ).astype(BF16)
    shares = jnp.dot(table, picks, preferred_element_type=F32).astype(BF16)
    row = iota((EXPERTS * 16, SLOTS + EXPERTS), 0)
    col = iota((EXPERTS * 16, SLOTS + EXPERTS), 1)
    source = row >> 4
    want = jnp.where(
        row - source * 16 < CAP,
        source * CAP + row - source * 16,
        jnp.where(row - source * 16 == CAP, SLOTS + source, -1),
    )
    place = jnp.where(col == want, 1.0, 0.0).astype(BF16)
    rows = jnp.dot(
        place, jnp.concatenate([total, shares], axis=0), preferred_element_type=F32
    )
    out_ref[...] = rows.astype(BF16).reshape(EXPERTS, 16, WIDTH)


def placed_rows(got):
    out = (pltpu.VMEM((EXPERTS, 16, WIDTH), BF16),)
    return kernel_call(place_kernel, out, "placed_rows", got)[0]


def combine_kernel(back_ref, rt_ref, gw_ref, out_ref, gate_ref):
    code, first, second = slot_codes(rt_ref[...])
    shape = (EXPERTS, 16, TOK)
    code3 = jnp.broadcast_to(code[:, None, :], shape)
    select = jnp.where(code3 == iota(shape, 1).astype(F32), 1.0, 0.0)
    select = select.reshape(EXPERTS * 16, TOK).T.astype(BF16)
    back = back_ref[...]
    rows = jnp.dot(
        select, back.reshape(EXPERTS * 16, WIDTH), preferred_element_type=F32
    )
    out_ref[...] = rows.astype(BF16)
    shares = back[:, CAP, 0:TOK].astype(F32)
    mine = jnp.zeros((EXPERTS, TOK), F32)
    for p in range(CAP):
        mine = mine + jnp.where(code == float(p), shares[:, p : p + 1], 0.0)
    top = jnp.sum(jnp.where(first, mine, 0.0), axis=0, keepdims=True)
    low = jnp.sum(jnp.where(second, mine, 0.0), axis=0, keepdims=True)
    gate_ref[...] = jnp.concatenate([top, low], axis=0) / gw_ref[...]


def combine(rt, gw, back):
    out = (
        jax.ShapeDtypeStruct((TOK, WIDTH), BF16),
        jax.ShapeDtypeStruct((TOP, TOK), F32),
    )
    return kernel_call(combine_kernel, out, "combine", rt, gw, near=(back,))


def core_swap(value):
    return lax.ppermute(value, "c", [(0, 1), (1, 0)])


def shards(tokens, cotangent, routes, gate_weight, w_gate, w_up, w_down, shared_hidden):
    rt, gw = routes.T, gate_weight.T
    core = lax.axis_index("c").astype(I32).reshape(1)
    wg, wu, wd = w_gate[0], w_up[0], w_down[0]
    sent = dispatch(rt, gw, tokens, cotangent)
    rows = lax.all_to_all(sent, EP, split_axis=0, concat_axis=0, tiled=True)
    rows, cotangent, wg, wu, wd = lax.optimization_barrier((rows, cotangent, wg, wu, wd))
    xg = lax.all_gather(rows.reshape(ROWS, WIDTH), "y", axis=0, tiled=False)

    wr = core_swap(other_half(core, wg, wu, wd))
    shared = lax.dot_general(
        shared_hidden, cotangent, (((0,), (0,)), ((), ())), preferred_element_type=F32
    ).astype(BF16)
    shared = lax.all_to_all(
        shared.reshape(EXPERTS, -1, WIDTH), EP, split_axis=0, concat_axis=0, tiled=True
    )
    shared_grad = jnp.sum(shared.astype(F32), axis=0)
    xg, wr, shared_grad = lax.optimization_barrier((xg, wr, shared_grad))

    own = forward(core, xg, wg, wu, wd, wr)
    parts, left = backward(core, own, core_swap(own), wg, wu, wr)
    got = lax.psum_scatter(parts, "y", scatter_dimension=0, tiled=False)
    theirs = core_swap(partner_grads(left, xg))
    grads = merged_grads(core, left, xg, theirs)
    got, *grads = lax.optimization_barrier((got, *grads))
    back = lax.all_to_all(placed_rows(got), EP, split_axis=0, concat_axis=0, tiled=True)
    tokens_grad, gate_grad = combine(rt, gw, back)
    return (tokens_grad, gate_grad.T, grads[0][None], grads[1][None], grads[2][None], shared_grad)


def solution(mesh):
    split = Mesh(mesh.devices.reshape(8, 4, 8, 2), ("z", "x", "y", "c"))
    ep, tp = ("z", "x"), ("y", "c")
    placed = (
        P(ep, tp),
        P(ep, tp),
        P(ep, None),
        P(ep, None),
        P(ep, tp, None),
        P(ep, tp, None),
        P(ep, tp, None),
        P(ep, None),
    )
    return jax.shard_map(
        shards,
        mesh=split,
        in_specs=placed,
        out_specs=(
            P(ep, tp),
            P(ep, None),
            P(ep, tp, None),
            P(ep, tp, None),
            P(ep, tp, None),
            P(ep, tp),
        ),
        check_vma=False,
    )
```

```python
import jax
import jax.numpy as jnp
from jax import lax
from jax.experimental import pallas as pl
from jax.experimental.pallas import tpu as pltpu
from jax.sharding import Mesh, PartitionSpec as P

TOK, TOP, EXPERTS, CAP = 128, 2, 32, 12
SLOTS = EXPERTS * CAP
ROWS = 2 * SLOTS
PAIR = 2 * CAP
WIDTH = 256
NY = 8
HALF = NY * WIDTH
HID = 64
BACK = SLOTS + 8
EP = ("z", "x")
F32, BF16, I32 = jnp.float32, jnp.bfloat16, jnp.int32


def iota(shape, dim):
    return lax.broadcasted_iota(I32, shape, dim)


def slot_codes(rt):
    ids = iota((EXPERTS, TOK), 0)
    first, second = rt[0:1, :] == ids, rt[1:2, :] == ids
    hot = jnp.where(first, 1.0, 0.0) + jnp.where(second, 1.0, 0.0)
    upper = jnp.where(iota((TOK, TOK), 0) < iota((TOK, TOK), 1), 1.0, 0.0)
    rank = jnp.dot(hot.astype(BF16), upper.astype(BF16), preferred_element_type=F32)
    return jnp.where(hot > 0.5, rank, -1.0), first, second


def dispatch_kernel(rt_ref, gw_ref, tok_ref, cot_ref, out_ref):
    code, first, second = slot_codes(rt_ref[...])
    gw = gw_ref[...]
    weight = jnp.where(first, gw[0:1, :], 0.0) + jnp.where(second, gw[1:2, :], 0.0)
    shape = (EXPERTS, PAIR, TOK)
    code3 = jnp.broadcast_to(code[:, None, :], shape)
    weight3 = jnp.broadcast_to(weight[:, None, :], shape)
    at = iota(shape, 1)
    atf = at.astype(F32)
    sel_x = jnp.where(code3 == atf, jnp.where(at < CAP, 1.0, 0.0), 0.0)
    sel_g = jnp.where(code3 == atf - float(CAP), jnp.where(at >= CAP, 1.0, 0.0), 0.0)
    scale = jnp.sum(sel_g * weight3 + sel_x, axis=2, keepdims=True).reshape(ROWS, 1)
    select = jnp.concatenate(
        [sel_x.reshape(ROWS, TOK).astype(BF16), sel_g.reshape(ROWS, TOK).astype(BF16)], axis=1
    )
    source = jnp.concatenate([tok_ref[...], cot_ref[...]], axis=0)
    rows = jnp.dot(select, source, preferred_element_type=F32)
    out_ref[...] = (rows * scale).astype(BF16).reshape(EXPERTS, PAIR, WIDTH)


def dispatch(rt, gw, tokens, cotangent):
    out = (pltpu.VMEM((EXPERTS, PAIR, WIDTH), BF16),)
    return kernel_call(dispatch_kernel, out, "dispatch", rt, gw, tokens, cotangent)[0]


def vmem(value):
    return pltpu.with_memory_space_constraint(value, pltpu.VMEM)


def kernel_call(body, out, name, *values, core=None, scratch=(), far=(), near=(), far_out=0):
    specs = [pl.BlockSpec(memory_space=pl.ANY)] * len(far)
    specs += [pl.BlockSpec(memory_space=pltpu.VMEM)] * len(near)
    specs += [pl.BlockSpec()] * len(values)
    values = [*far, *(vmem(v) for v in near), *values]
    if core is not None:
        specs, values = [pl.BlockSpec(memory_space=pltpu.SMEM)] + specs, [core] + values
    results = [
        pl.BlockSpec(memory_space=pl.ANY)
        if at < far_out
        else pl.BlockSpec()
        if isinstance(shape, jax.ShapeDtypeStruct)
        else pl.BlockSpec(memory_space=pltpu.VMEM)
        for at, shape in enumerate(out)
    ]
    return pl.pallas_call(
        body,
        in_specs=specs,
        out_specs=results,
        out_shape=list(out),
        scratch_shapes=list(scratch),
        name=name,
    )(*values)


def fetch(pairs, sems):
    copies = [
        pltpu.make_async_copy(there, here, sems.at[at]) for at, (there, here) in enumerate(pairs)
    ]
    for copy in copies:
        copy.start()
    return copies


def flags(count):
    return pltpu.SemaphoreType.DMA((count,))


def lanes_of(step, half):
    return pl.ds(pl.multiple_of((2 * step + half) * WIDTH, WIDTH), WIDTH)


def half_lanes(y):
    return slice(y * WIDTH, (y + 1) * WIDTH)


def split_kernel(c_ref, wg_ref, wu_ref, wd_ref, out_ref):
    for at, ref in enumerate((wg_ref, wu_ref, wd_ref)):
        for y in range(NY):
            out_ref[at, :, half_lanes(y)] = ref[:, lanes_of(y, 1 - c_ref[0])]


def other_half(core, wg, wu, wd):
    out = (jax.ShapeDtypeStruct((3, HID, HALF), BF16),)
    return kernel_call(split_kernel, out, "other_half", wg, wu, wd, core=core)[0]


def is_token_lane(shape):
    lane = iota(shape, 1)
    return lane - ((lane * 2731) >> 16) * PAIR < CAP


def forward_kernel(
    c_ref, xg_far, wg_far, wu_far, wd_far, wr_far, out_ref, xg_ref, own_ref, wr_ref, sems
):
    pairs = []
    for y in range(NY):
        pairs.append((xg_far.at[y], xg_ref.at[y]))
        pairs.append((wr_far.at[:, :, half_lanes(y)], wr_ref.at[:, :, half_lanes(y)]))
        for at, far in enumerate((wg_far, wu_far, wd_far)):
            pairs.append((far.at[:, lanes_of(y, c_ref[0])], own_ref.at[at, :, half_lanes(y)]))
    copies = fetch(pairs, sems)
    total = None
    for y in range(NY):
        for copy in copies[5 * y : 5 * y + 5]:
            copy.wait()
        parts = []
        for at in (0, 2, 1):
            parts.append(own_ref[at, :, half_lanes(y)])
            parts.append(wr_ref[at, :, half_lanes(y)])
        part = lax.dot_general(
            jnp.concatenate(parts, axis=0),
            xg_ref[y],
            (((1,), (1,)), ((), ())),
            preferred_element_type=F32,
        )
        total = part if total is None else total + part
    pair = 2 * HID
    out_ref[0:pair, :] = jnp.where(
        is_token_lane((pair, ROWS)), total[0:pair, :], total[pair : 2 * pair, :]
    ).astype(BF16)
    out_ref[pair : 2 * pair, :] = total[2 * pair : 3 * pair, :].astype(BF16)


def forward(core, xg, wg, wu, wd, wr):
    out = (pltpu.VMEM((4 * HID, ROWS), BF16),)
    return kernel_call(
        forward_kernel,
        out,
        "forward",
        core=core,
        far=(xg, wg, wu, wd, wr),
        scratch=(
            pltpu.VMEM((NY, ROWS, WIDTH), BF16),
            pltpu.VMEM((3, HID, HALF), BF16),
            pltpu.VMEM((3, HID, HALF), BF16),
            flags(5 * NY),
        ),
    )[0]


def backward_kernel(
    c_ref, wg_far, wu_far, wr_far, own_ref, got_ref, out_far, left_ref,
    wg_ref, wu_ref, wr_ref, out_ref, sems, out_sems,
):
    copies = fetch(
        [
            (wg_far, wg_ref),
            (wu_far, wu_ref),
            (wr_far.at[0:2], wr_ref),
        ],
        sems,
    )

    def total(at):
        low, mid, high = 2 * at * HID, (2 * at + 1) * HID, (2 * at + 2) * HID
        return jnp.concatenate(
            [
                own_ref[low:mid, :].astype(F32) + got_ref[mid:high, :].astype(F32),
                own_ref[mid:high, :].astype(F32) + got_ref[low:mid, :].astype(F32),
            ],
            axis=0,
        )

    pre_gate, pre_up = total(0), total(1)
    keep = is_token_lane((2 * HID, ROWS))
    back = pltpu.roll(pre_gate, ROWS - CAP, 1)
    sig = 1.0 / (1.0 + jnp.exp(-jnp.where(keep, pre_gate, 0.0)))
    silu = pre_gate * sig
    hidden = jnp.where(keep, silu * pre_up, 0.0).astype(BF16).astype(F32)
    grad_gate = jnp.where(keep, back * pre_up * sig * (1.0 + pre_gate * (1.0 - sig)), 0.0)
    grad_up = jnp.where(keep, back * silu, 0.0)
    gate = jnp.sum(hidden * back, axis=0, keepdims=True)
    upper = gate.astype(BF16).astype(F32)
    tail = [part[:, half_lanes(at)] for part in (upper, gate - upper) for at in range(3)]
    tail = jnp.concatenate(tail + [jnp.zeros((2, WIDTH), F32)], axis=0).astype(BF16)
    shifted = pltpu.roll(hidden, CAP, 1)
    for at, grad in enumerate((grad_gate, grad_up, shifted)):
        grad = grad.astype(BF16)
        left_ref[0, at * HID : (at + 1) * HID, :] = grad[0:HID]
        left_ref[1, at * HID : (at + 1) * HID, :] = grad[HID : 2 * HID]
    both = jnp.concatenate([grad_gate.astype(BF16), grad_up.astype(BF16)], axis=0)
    slot = iota((SLOTS, ROWS), 0)
    lane = iota((SLOTS, ROWS), 1)
    compact = jnp.where(lane == slot + ((slot * 5462) >> 16) * CAP, 1.0, 0.0).astype(BF16)
    grads = lax.dot_general(
        compact, both, (((1,), (1,)), ((), ())), preferred_element_type=F32
    ).astype(BF16)
    for copy in copies:
        copy.wait()
    sent = []
    for y in range(NY):
        mats = jnp.concatenate(
            [
                wg_ref[:, lanes_of(y, c_ref[0])],
                wr_ref[0, :, half_lanes(y)],
                wu_ref[:, lanes_of(y, c_ref[0])],
                wr_ref[1, :, half_lanes(y)],
            ],
            axis=0,
        )
        out_ref[y, 0:SLOTS, :] = jnp.dot(grads, mats, preferred_element_type=F32).astype(BF16)
        out_ref[y, SLOTS:BACK, :] = tail
        sent.append(pltpu.make_async_copy(out_ref.at[y], out_far.at[y], out_sems.at[y]))
        sent[y].start()
    for copy in sent:
        copy.wait()


def backward(core, own, got, wg, wu, wr):
    out = (
        jax.ShapeDtypeStruct((NY, BACK, WIDTH), BF16),
        jax.ShapeDtypeStruct((2, 3 * HID, ROWS), BF16),
    )
    return kernel_call(
        backward_kernel,
        out,
        "backward",
        core=core,
        far=(wg, wu, wr),
        near=(own, got),
        far_out=1,
        scratch=(
            pltpu.VMEM((HID, 2 * HALF), BF16),
            pltpu.VMEM((HID, 2 * HALF), BF16),
            pltpu.VMEM((2, HID, HALF), BF16),
            pltpu.VMEM((NY, BACK, WIDTH), BF16),
            flags(3),
            flags(NY),
        ),
    )


def partner_kernel(left_far, xg_far, out_ref, left_ref, xg_ref, sems):
    copies = fetch(
        [(left_far.at[1], left_ref)] + [(xg_far.at[y], xg_ref.at[y]) for y in range(NY)], sems
    )
    copies[0].wait()
    for y in range(NY):
        copies[1 + y].wait()
        out_ref[:, half_lanes(y)] = jnp.dot(
            left_ref[...], xg_ref[y], preferred_element_type=F32
        ).astype(BF16)


def partner_grads(left, xg):
    return kernel_call(
        partner_kernel,
        (jax.ShapeDtypeStruct((3 * HID, HALF), BF16),),
        "partner_grads",
        far=(left, xg),
        scratch=(
            pltpu.VMEM((3 * HID, ROWS), BF16),
            pltpu.VMEM((NY, ROWS, WIDTH), BF16),
            flags(1 + NY),
        ),
    )[0]


def merge_kernel(
    c_ref, left_far, xg_far, got_far, gate_far, up_far, down_far, left_ref, xg_ref, got_ref, out_ref, sems, out_sems
):
    copies = fetch(
        [(left_far.at[0], left_ref), (got_far, got_ref)]
        + [(xg_far.at[y], xg_ref.at[y]) for y in range(NY)],
        sems,
    )
    copies[0].wait()
    copies[1].wait()
    sent = []
    for y in range(NY):
        copies[2 + y].wait()
        mine = jnp.dot(left_ref[...], xg_ref[y], preferred_element_type=F32)
        theirs = got_ref[:, half_lanes(y)].astype(F32)
        both = slice(2 * y * WIDTH, (2 * y + 2) * WIDTH)
        for at, far in enumerate((gate_far, up_far, down_far)):
            rows = slice(at * HID, (at + 1) * HID)
            out_ref[at, :, lanes_of(y, c_ref[0])] = mine[rows, :]
            out_ref[at, :, lanes_of(y, 1 - c_ref[0])] = theirs[rows, :]
            sent.append(
                pltpu.make_async_copy(
                    out_ref.at[at, :, both], far.at[:, both], out_sems.at[3 * y + at]
                )
            )
            sent[-1].start()
    for copy in sent:
        copy.wait()


def merged_grads(core, left, xg, got):
    return kernel_call(
        merge_kernel,
        [jax.ShapeDtypeStruct((HID, 2 * HALF), F32)] * 3,
        "merged_grads",
        core=core,
        far=(left, xg, got),
        far_out=3,
        scratch=(
            pltpu.VMEM((3 * HID, ROWS), BF16),
            pltpu.VMEM((NY, ROWS, WIDTH), BF16),
            pltpu.VMEM((3 * HID, HALF), BF16),
            pltpu.VMEM((3, HID, 2 * HALF), F32),
            flags(2 + NY),
            flags(3 * NY),
        ),
    )


def place_kernel(got_ref, out_ref):
    total = got_ref[...].astype(F32)
    gate = total[SLOTS : SLOTS + 3, :] + total[SLOTS + 3 : SLOTS + 6, :]
    gate = jnp.concatenate([gate[at : at + 1, :] for at in range(3)], axis=1)
    total = total[0:SLOTS, :].astype(BF16)
    src = iota((EXPERTS, ROWS), 0)
    lane = iota((EXPERTS, ROWS), 1)
    table = jnp.where(
        (lane * 2731) >> 16 == src, jnp.broadcast_to(gate, (EXPERTS, ROWS)), 0.0
    ).astype(BF16)
    at = iota((ROWS, WIDTH), 0)
    picks = jnp.where(
        at - ((at * 2731) >> 16) * PAIR == iota((ROWS, WIDTH), 1), 1.0, 0.0
    ).astype(BF16)
    shares = jnp.dot(table, picks, preferred_element_type=F32).astype(BF16)
    row = iota((EXPERTS * 16, SLOTS + EXPERTS), 0)
    col = iota((EXPERTS * 16, SLOTS + EXPERTS), 1)
    source = row >> 4
    want = jnp.where(
        row - source * 16 < CAP,
        source * CAP + row - source * 16,
        jnp.where(row - source * 16 == CAP, SLOTS + source, -1),
    )
    place = jnp.where(col == want, 1.0, 0.0).astype(BF16)
    rows = jnp.dot(
        place, jnp.concatenate([total, shares], axis=0), preferred_element_type=F32
    )
    out_ref[...] = rows.astype(BF16).reshape(EXPERTS, 16, WIDTH)


def placed_rows(got):
    out = (pltpu.VMEM((EXPERTS, 16, WIDTH), BF16),)
    return kernel_call(place_kernel, out, "placed_rows", got)[0]


def combine_kernel(back_ref, rt_ref, gw_ref, out_ref, gate_ref):
    code, first, second = slot_codes(rt_ref[...])
    shape = (EXPERTS, 16, TOK)
    code3 = jnp.broadcast_to(code[:, None, :], shape)
    select = jnp.where(code3 == iota(shape, 1).astype(F32), 1.0, 0.0)
    select = select.reshape(EXPERTS * 16, TOK).T.astype(BF16)
    back = back_ref[...]
    rows = jnp.dot(
        select, back.reshape(EXPERTS * 16, WIDTH), preferred_element_type=F32
    )
    out_ref[...] = rows.astype(BF16)
    shares = back[:, CAP, 0:TOK].astype(F32)
    mine = jnp.zeros((EXPERTS, TOK), F32)
    for p in range(CAP):
        mine = mine + jnp.where(code == float(p), shares[:, p : p + 1], 0.0)
    top = jnp.sum(jnp.where(first, mine, 0.0), axis=0, keepdims=True)
    low = jnp.sum(jnp.where(second, mine, 0.0), axis=0, keepdims=True)
    gate_ref[...] = jnp.concatenate([top, low], axis=0) / gw_ref[...]


def combine(rt, gw, back):
    out = (
        jax.ShapeDtypeStruct((TOK, WIDTH), BF16),
        jax.ShapeDtypeStruct((TOP, TOK), F32),
    )
    return kernel_call(combine_kernel, out, "combine", rt, gw, near=(back,))


def core_swap(value):
    return lax.ppermute(value, "c", [(0, 1), (1, 0)])


def shards(tokens, cotangent, routes, gate_weight, w_gate, w_up, w_down, shared_hidden):
    rt, gw = routes.T, gate_weight.T
    core = lax.axis_index("c").astype(I32).reshape(1)
    wg, wu, wd = w_gate[0], w_up[0], w_down[0]
    sent = dispatch(rt, gw, tokens, cotangent)
    rows = lax.all_to_all(sent, EP, split_axis=0, concat_axis=0, tiled=True)
    rows, cotangent, wg, wu, wd = lax.optimization_barrier((rows, cotangent, wg, wu, wd))
    xg = lax.all_gather(rows.reshape(ROWS, WIDTH), "y", axis=0, tiled=False)

    wr = core_swap(other_half(core, wg, wu, wd))
    shared = lax.dot_general(
        shared_hidden, cotangent, (((0,), (0,)), ((), ())), preferred_element_type=F32
    ).astype(BF16)
    shared = lax.all_to_all(
        shared.reshape(EXPERTS, -1, WIDTH), EP, split_axis=0, concat_axis=0, tiled=True
    )
    shared_grad = jnp.sum(shared.astype(F32), axis=0)
    xg, wr, shared_grad = lax.optimization_barrier((xg, wr, shared_grad))

    own = forward(core, xg, wg, wu, wd, wr)
    parts, left = backward(core, own, core_swap(own), wg, wu, wr)
    got = lax.psum_scatter(parts, "y", scatter_dimension=0, tiled=False)
    theirs = core_swap(partner_grads(left, xg))
    grads = merged_grads(core, left, xg, theirs)
    got, *grads = lax.optimization_barrier((got, *grads))
    back = lax.all_to_all(placed_rows(got), EP, split_axis=0, concat_axis=0, tiled=True)
    tokens_grad, gate_grad = combine(rt, gw, back)
    return (tokens_grad, gate_grad.T, grads[0][None], grads[1][None], grads[2][None], shared_grad)


def solution(mesh):
    split = Mesh(mesh.devices.reshape(8, 4, 8, 2), ("z", "x", "y", "c"))
    ep, tp = ("z", "x"), ("y", "c")
    placed = (
        P(ep, tp),
        P(ep, tp),
        P(ep, None),
        P(ep, None),
        P(ep, tp, None),
        P(ep, tp, None),
        P(ep, tp, None),
        P(ep, None),
    )
    return jax.shard_map(
        shards,
        mesh=split,
        in_specs=placed,
        out_specs=(
            P(ep, tp),
            P(ep, None),
            P(ep, tp, None),
            P(ep, tp, None),
            P(ep, tp, None),
            P(ep, tp),
        ),
        check_vma=False,
    )
```

```python
import jax
import jax.numpy as jnp
from jax import lax
from jax.experimental import pallas as pl
from jax.experimental.pallas import tpu as pltpu
from jax.sharding import Mesh, PartitionSpec as P

TOK, TOP, EXPERTS, CAP = 128, 2, 32, 12
SLOTS = EXPERTS * CAP
ROWS = 2 * SLOTS
PAIR = 2 * CAP
WIDTH = 256
NY = 8
HALF = NY * WIDTH
HID = 64
BACK = SLOTS + 8
EP = ("z", "x")
F32, BF16, I32 = jnp.float32, jnp.bfloat16, jnp.int32


def iota(shape, dim):
    return lax.broadcasted_iota(I32, shape, dim)


def slot_codes(rt):
    ids = iota((EXPERTS, TOK), 0)
    first, second = rt[0:1, :] == ids, rt[1:2, :] == ids
    hot = jnp.where(first, 1.0, 0.0) + jnp.where(second, 1.0, 0.0)
    upper = jnp.where(iota((TOK, TOK), 0) < iota((TOK, TOK), 1), 1.0, 0.0)
    rank = jnp.dot(hot.astype(BF16), upper.astype(BF16), preferred_element_type=F32)
    return jnp.where(hot > 0.5, rank, -1.0), first, second


def dispatch_kernel(rt_ref, gw_ref, tok_ref, cot_ref, out_ref):
    code, first, second = slot_codes(rt_ref[...])
    gw = gw_ref[...]
    weight = jnp.where(first, gw[0:1, :], 0.0) + jnp.where(second, gw[1:2, :], 0.0)
    shape = (EXPERTS, PAIR, TOK)
    code3 = jnp.broadcast_to(code[:, None, :], shape)
    weight3 = jnp.broadcast_to(weight[:, None, :], shape)
    at = iota(shape, 1)
    atf = at.astype(F32)
    sel_x = jnp.where(code3 == atf, jnp.where(at < CAP, 1.0, 0.0), 0.0)
    sel_g = jnp.where(code3 == atf - float(CAP), jnp.where(at >= CAP, 1.0, 0.0), 0.0)
    scale = jnp.sum(sel_g * weight3 + sel_x, axis=2, keepdims=True).reshape(ROWS, 1)
    select = jnp.concatenate(
        [sel_x.reshape(ROWS, TOK).astype(BF16), sel_g.reshape(ROWS, TOK).astype(BF16)], axis=1
    )
    source = jnp.concatenate([tok_ref[...], cot_ref[...]], axis=0)
    rows = jnp.dot(select, source, preferred_element_type=F32)
    out_ref[...] = (rows * scale).astype(BF16).reshape(EXPERTS, PAIR, WIDTH)


def dispatch(rt, gw, tokens, cotangent):
    out = (pltpu.VMEM((EXPERTS, PAIR, WIDTH), BF16),)
    return kernel_call(dispatch_kernel, out, "dispatch", rt, gw, tokens, cotangent)[0]


def vmem(value):
    return pltpu.with_memory_space_constraint(value, pltpu.VMEM)


def kernel_call(body, out, name, *values, core=None, scratch=(), far=(), near=(), far_out=0):
    specs = [pl.BlockSpec(memory_space=pl.ANY)] * len(far)
    specs += [pl.BlockSpec(memory_space=pltpu.VMEM)] * len(near)
    specs += [pl.BlockSpec()] * len(values)
    values = [*far, *(vmem(v) for v in near), *values]
    if core is not None:
        specs, values = [pl.BlockSpec(memory_space=pltpu.SMEM)] + specs, [core] + values
    results = [
        pl.BlockSpec(memory_space=pl.ANY)
        if at < far_out
        else pl.BlockSpec()
        if isinstance(shape, jax.ShapeDtypeStruct)
        else pl.BlockSpec(memory_space=pltpu.VMEM)
        for at, shape in enumerate(out)
    ]
    return pl.pallas_call(
        body,
        in_specs=specs,
        out_specs=results,
        out_shape=list(out),
        scratch_shapes=list(scratch),
        name=name,
    )(*values)


def fetch(pairs, sems):
    copies = [
        pltpu.make_async_copy(there, here, sems.at[at]) for at, (there, here) in enumerate(pairs)
    ]
    for copy in copies:
        copy.start()
    return copies


def flags(count):
    return pltpu.SemaphoreType.DMA((count,))


def lanes_of(step, half):
    return pl.ds(pl.multiple_of((2 * step + half) * WIDTH, WIDTH), WIDTH)


def half_lanes(y):
    return slice(y * WIDTH, (y + 1) * WIDTH)


def split_kernel(c_ref, wg_ref, wu_ref, wd_ref, out_ref):
    for at, ref in enumerate((wg_ref, wu_ref, wd_ref)):
        for y in range(NY):
            out_ref[at, :, half_lanes(y)] = ref[:, lanes_of(y, 1 - c_ref[0])]


def other_half(core, wg, wu, wd):
    out = (jax.ShapeDtypeStruct((3, HID, HALF), BF16),)
    return kernel_call(split_kernel, out, "other_half", wg, wu, wd, core=core)[0]


def is_token_lane(shape):
    lane = iota(shape, 1)
    return lane - ((lane * 2731) >> 16) * PAIR < CAP


def forward_kernel(
    c_ref, xg_far, wg_far, wu_far, wd_far, wr_far, out_ref, xg_ref, own_ref, wr_ref, sems
):
    pairs = []
    for y in range(NY):
        pairs.append((xg_far.at[y], xg_ref.at[y]))
        pairs.append((wr_far.at[:, :, half_lanes(y)], wr_ref.at[:, :, half_lanes(y)]))
        for at, far in enumerate((wg_far, wu_far, wd_far)):
            pairs.append((far.at[:, lanes_of(y, c_ref[0])], own_ref.at[at, :, half_lanes(y)]))
    copies = fetch(pairs, sems)
    total = None
    for y in range(NY):
        for copy in copies[5 * y : 5 * y + 5]:
            copy.wait()
        parts = []
        for at in (0, 2, 1):
            parts.append(own_ref[at, :, half_lanes(y)])
            parts.append(wr_ref[at, :, half_lanes(y)])
        part = lax.dot_general(
            jnp.concatenate(parts, axis=0),
            xg_ref[y],
            (((1,), (1,)), ((), ())),
            preferred_element_type=F32,
        )
        total = part if total is None else total + part
    pair = 2 * HID
    out_ref[0:pair, :] = jnp.where(
        is_token_lane((pair, ROWS)), total[0:pair, :], total[pair : 2 * pair, :]
    ).astype(BF16)
    out_ref[pair : 2 * pair, :] = total[2 * pair : 3 * pair, :].astype(BF16)


def forward(core, xg, wg, wu, wd, wr):
    out = (pltpu.VMEM((4 * HID, ROWS), BF16),)
    return kernel_call(
        forward_kernel,
        out,
        "forward",
        core=core,
        far=(xg, wg, wu, wd, wr),
        scratch=(
            pltpu.VMEM((NY, ROWS, WIDTH), BF16),
            pltpu.VMEM((3, HID, HALF), BF16),
            pltpu.VMEM((3, HID, HALF), BF16),
            flags(5 * NY),
        ),
    )[0]


def backward_kernel(
    c_ref, wg_far, wu_far, wr_far, own_ref, got_ref, out_far, left_far,
    wg_ref, wu_ref, wr_ref, out_ref, left_ref, sems, out_sems,
):
    copies = fetch(
        [
            (wg_far, wg_ref),
            (wu_far, wu_ref),
            (wr_far.at[0:2], wr_ref),
        ],
        sems,
    )

    def total(at):
        low, mid, high = 2 * at * HID, (2 * at + 1) * HID, (2 * at + 2) * HID
        return jnp.concatenate(
            [
                own_ref[low:mid, :].astype(F32) + got_ref[mid:high, :].astype(F32),
                own_ref[mid:high, :].astype(F32) + got_ref[low:mid, :].astype(F32),
            ],
            axis=0,
        )

    pre_gate, pre_up = total(0), total(1)
    keep = is_token_lane((2 * HID, ROWS))
    back = pltpu.roll(pre_gate, ROWS - CAP, 1)
    sig = 1.0 / (1.0 + jnp.exp(-jnp.where(keep, pre_gate, 0.0)))
    silu = pre_gate * sig
    hidden = jnp.where(keep, silu * pre_up, 0.0).astype(BF16).astype(F32)
    grad_gate = jnp.where(keep, back * pre_up * sig * (1.0 + pre_gate * (1.0 - sig)), 0.0)
    grad_up = jnp.where(keep, back * silu, 0.0)
    gate = jnp.sum(hidden * back, axis=0, keepdims=True)
    upper = gate.astype(BF16).astype(F32)
    tail = [part[:, half_lanes(at)] for part in (upper, gate - upper) for at in range(3)]
    tail = jnp.concatenate(tail + [jnp.zeros((2, WIDTH), F32)], axis=0).astype(BF16)
    shifted = pltpu.roll(hidden, CAP, 1)
    for at, grad in enumerate((grad_gate, grad_up, shifted)):
        grad = grad.astype(BF16)
        left_ref[0, at * HID : (at + 1) * HID, :] = grad[0:HID]
        left_ref[1, at * HID : (at + 1) * HID, :] = grad[HID : 2 * HID]
    sent = [pltpu.make_async_copy(left_ref, left_far, out_sems.at[NY])]
    sent[0].start()
    both = jnp.concatenate([grad_gate.astype(BF16), grad_up.astype(BF16)], axis=0)
    slot = iota((SLOTS, ROWS), 0)
    lane = iota((SLOTS, ROWS), 1)
    compact = jnp.where(lane == slot + ((slot * 5462) >> 16) * CAP, 1.0, 0.0).astype(BF16)
    grads = lax.dot_general(
        compact, both, (((1,), (1,)), ((), ())), preferred_element_type=F32
    ).astype(BF16)
    for copy in copies:
        copy.wait()
    for y in range(NY):
        mats = jnp.concatenate(
            [
                wg_ref[:, lanes_of(y, c_ref[0])],
                wr_ref[0, :, half_lanes(y)],
                wu_ref[:, lanes_of(y, c_ref[0])],
                wr_ref[1, :, half_lanes(y)],
            ],
            axis=0,
        )
        out_ref[y, 0:SLOTS, :] = jnp.dot(grads, mats, preferred_element_type=F32).astype(BF16)
        out_ref[y, SLOTS:BACK, :] = tail
        sent.append(pltpu.make_async_copy(out_ref.at[y], out_far.at[y], out_sems.at[y]))
        sent[-1].start()
    for copy in sent:
        copy.wait()


def backward(core, own, got, wg, wu, wr):
    out = (
        jax.ShapeDtypeStruct((NY, BACK, WIDTH), BF16),
        jax.ShapeDtypeStruct((2, 3 * HID, ROWS), BF16),
    )
    return kernel_call(
        backward_kernel,
        out,
        "backward",
        core=core,
        far=(wg, wu, wr),
        near=(own, got),
        far_out=2,
        scratch=(
            pltpu.VMEM((HID, 2 * HALF), BF16),
            pltpu.VMEM((HID, 2 * HALF), BF16),
            pltpu.VMEM((2, HID, HALF), BF16),
            pltpu.VMEM((NY, BACK, WIDTH), BF16),
            pltpu.VMEM((2, 3 * HID, ROWS), BF16),
            flags(3),
            flags(NY + 1),
        ),
    )


def partner_kernel(left_far, xg_far, out_ref, left_ref, xg_ref, sems):
    copies = fetch(
        [(left_far.at[1], left_ref)] + [(xg_far.at[y], xg_ref.at[y]) for y in range(NY)], sems
    )
    copies[0].wait()
    for y in range(NY):
        copies[1 + y].wait()
        out_ref[:, half_lanes(y)] = jnp.dot(
            left_ref[...], xg_ref[y], preferred_element_type=F32
        ).astype(BF16)


def partner_grads(left, xg):
    return kernel_call(
        partner_kernel,
        (jax.ShapeDtypeStruct((3 * HID, HALF), BF16),),
        "partner_grads",
        far=(left, xg),
        scratch=(
            pltpu.VMEM((3 * HID, ROWS), BF16),
            pltpu.VMEM((NY, ROWS, WIDTH), BF16),
            flags(1 + NY),
        ),
    )[0]


def merge_kernel(
    c_ref, left_far, xg_far, got_far, gate_far, up_far, down_far, left_ref, xg_ref, got_ref, out_ref, sems, out_sems
):
    copies = fetch(
        [(left_far.at[0], left_ref), (got_far, got_ref)]
        + [(xg_far.at[y], xg_ref.at[y]) for y in range(NY)],
        sems,
    )
    copies[0].wait()
    copies[1].wait()
    sent = []
    for y in range(NY):
        copies[2 + y].wait()
        mine = jnp.dot(left_ref[...], xg_ref[y], preferred_element_type=F32)
        theirs = got_ref[:, half_lanes(y)].astype(F32)
        both = slice(2 * y * WIDTH, (2 * y + 2) * WIDTH)
        for at, far in enumerate((gate_far, up_far, down_far)):
            rows = slice(at * HID, (at + 1) * HID)
            out_ref[at, :, lanes_of(y, c_ref[0])] = mine[rows, :]
            out_ref[at, :, lanes_of(y, 1 - c_ref[0])] = theirs[rows, :]
            sent.append(
                pltpu.make_async_copy(
                    out_ref.at[at, :, both], far.at[:, both], out_sems.at[3 * y + at]
                )
            )
            sent[-1].start()
    for copy in sent:
        copy.wait()


def merged_grads(core, left, xg, got):
    return kernel_call(
        merge_kernel,
        [jax.ShapeDtypeStruct((HID, 2 * HALF), F32)] * 3,
        "merged_grads",
        core=core,
        far=(left, xg, got),
        far_out=3,
        scratch=(
            pltpu.VMEM((3 * HID, ROWS), BF16),
            pltpu.VMEM((NY, ROWS, WIDTH), BF16),
            pltpu.VMEM((3 * HID, HALF), BF16),
            pltpu.VMEM((3, HID, 2 * HALF), F32),
            flags(2 + NY),
            flags(3 * NY),
        ),
    )


def place_kernel(got_ref, out_ref):
    total = got_ref[...].astype(F32)
    gate = total[SLOTS : SLOTS + 3, :] + total[SLOTS + 3 : SLOTS + 6, :]
    gate = jnp.concatenate([gate[at : at + 1, :] for at in range(3)], axis=1)
    total = total[0:SLOTS, :].astype(BF16)
    src = iota((EXPERTS, ROWS), 0)
    lane = iota((EXPERTS, ROWS), 1)
    table = jnp.where(
        (lane * 2731) >> 16 == src, jnp.broadcast_to(gate, (EXPERTS, ROWS)), 0.0
    ).astype(BF16)
    at = iota((ROWS, WIDTH), 0)
    picks = jnp.where(
        at - ((at * 2731) >> 16) * PAIR == iota((ROWS, WIDTH), 1), 1.0, 0.0
    ).astype(BF16)
    shares = jnp.dot(table, picks, preferred_element_type=F32).astype(BF16)
    row = iota((EXPERTS * 16, SLOTS + EXPERTS), 0)
    col = iota((EXPERTS * 16, SLOTS + EXPERTS), 1)
    source = row >> 4
    want = jnp.where(
        row - source * 16 < CAP,
        source * CAP + row - source * 16,
        jnp.where(row - source * 16 == CAP, SLOTS + source, -1),
    )
    place = jnp.where(col == want, 1.0, 0.0).astype(BF16)
    rows = jnp.dot(
        place, jnp.concatenate([total, shares], axis=0), preferred_element_type=F32
    )
    out_ref[...] = rows.astype(BF16).reshape(EXPERTS, 16, WIDTH)


def placed_rows(got):
    out = (pltpu.VMEM((EXPERTS, 16, WIDTH), BF16),)
    return kernel_call(place_kernel, out, "placed_rows", got)[0]


def combine_kernel(back_ref, rt_ref, gw_ref, out_ref, gate_ref):
    code, first, second = slot_codes(rt_ref[...])
    shape = (EXPERTS, 16, TOK)
    code3 = jnp.broadcast_to(code[:, None, :], shape)
    select = jnp.where(code3 == iota(shape, 1).astype(F32), 1.0, 0.0)
    select = select.reshape(EXPERTS * 16, TOK).T.astype(BF16)
    back = back_ref[...]
    rows = jnp.dot(
        select, back.reshape(EXPERTS * 16, WIDTH), preferred_element_type=F32
    )
    out_ref[...] = rows.astype(BF16)
    shares = back[:, CAP, 0:TOK].astype(F32)
    mine = jnp.zeros((EXPERTS, TOK), F32)
    for p in range(CAP):
        mine = mine + jnp.where(code == float(p), shares[:, p : p + 1], 0.0)
    top = jnp.sum(jnp.where(first, mine, 0.0), axis=0, keepdims=True)
    low = jnp.sum(jnp.where(second, mine, 0.0), axis=0, keepdims=True)
    gate_ref[...] = jnp.concatenate([top, low], axis=0) / gw_ref[...]


def combine(rt, gw, back):
    out = (
        jax.ShapeDtypeStruct((TOK, WIDTH), BF16),
        jax.ShapeDtypeStruct((TOP, TOK), F32),
    )
    return kernel_call(combine_kernel, out, "combine", near=(back, rt, gw))


def core_swap(value):
    return lax.ppermute(value, "c", [(0, 1), (1, 0)])


def shards(tokens, cotangent, routes, gate_weight, w_gate, w_up, w_down, shared_hidden):
    rt, gw = routes.T, gate_weight.T
    core = lax.axis_index("c").astype(I32).reshape(1)
    wg, wu, wd = w_gate[0], w_up[0], w_down[0]
    sent = dispatch(rt, gw, tokens, cotangent)
    rows = lax.all_to_all(sent, EP, split_axis=0, concat_axis=0, tiled=True)
    rows, cotangent, wg, wu, wd = lax.optimization_barrier((rows, cotangent, wg, wu, wd))
    xg = lax.all_gather(rows.reshape(ROWS, WIDTH), "y", axis=0, tiled=False)

    wr = core_swap(other_half(core, wg, wu, wd))
    shared = lax.dot_general(
        shared_hidden, cotangent, (((0,), (0,)), ((), ())), preferred_element_type=F32
    ).astype(BF16)
    shared = lax.all_to_all(
        shared.reshape(EXPERTS, -1, WIDTH), EP, split_axis=0, concat_axis=0, tiled=True
    )
    shared_grad = jnp.sum(shared.astype(F32), axis=0)
    xg, wr, shared_grad = lax.optimization_barrier((xg, wr, shared_grad))

    own = forward(core, xg, wg, wu, wd, wr)
    parts, left = backward(core, own, core_swap(own), wg, wu, wr)
    got = lax.psum_scatter(parts, "y", scatter_dimension=0, tiled=False)
    theirs = core_swap(partner_grads(left, xg))
    grads = merged_grads(core, left, xg, theirs)
    got, *grads = lax.optimization_barrier((got, *grads))
    back = lax.all_to_all(placed_rows(got), EP, split_axis=0, concat_axis=0, tiled=True)
    tokens_grad, gate_grad = combine(rt, gw, back)
    return (tokens_grad, gate_grad.T, grads[0][None], grads[1][None], grads[2][None], shared_grad)


def solution(mesh):
    split = Mesh(mesh.devices.reshape(8, 4, 8, 2), ("z", "x", "y", "c"))
    ep, tp = ("z", "x"), ("y", "c")
    placed = (
        P(ep, tp),
        P(ep, tp),
        P(ep, None),
        P(ep, None),
        P(ep, tp, None),
        P(ep, tp, None),
        P(ep, tp, None),
        P(ep, None),
    )
    return jax.shard_map(
        shards,
        mesh=split,
        in_specs=placed,
        out_specs=(
            P(ep, tp),
            P(ep, None),
            P(ep, tp, None),
            P(ep, tp, None),
            P(ep, tp, None),
            P(ep, tp),
        ),
        check_vma=False,
    )
```

```python
import jax
import jax.numpy as jnp
from jax import lax
from jax.experimental import pallas as pl
from jax.experimental.pallas import tpu as pltpu
from jax.sharding import Mesh, PartitionSpec as P

TOK, TOP, EXPERTS, CAP = 128, 2, 32, 12
SLOTS = EXPERTS * CAP
ROWS = 2 * SLOTS
PAIR = 2 * CAP
WIDTH = 256
NY = 8
HALF = NY * WIDTH
HID = 64
BACK = SLOTS + 8
EP = ("z", "x")
F32, BF16, I32 = jnp.float32, jnp.bfloat16, jnp.int32


def iota(shape, dim):
    return lax.broadcasted_iota(I32, shape, dim)


def slot_codes(rt):
    ids = iota((EXPERTS, TOK), 0)
    first, second = rt[0:1, :] == ids, rt[1:2, :] == ids
    hot = jnp.where(first, 1.0, 0.0) + jnp.where(second, 1.0, 0.0)
    upper = jnp.where(iota((TOK, TOK), 0) < iota((TOK, TOK), 1), 1.0, 0.0)
    rank = jnp.dot(hot.astype(BF16), upper.astype(BF16), preferred_element_type=F32)
    return jnp.where(hot > 0.5, rank, -1.0), first, second


def dispatch_kernel(rt_ref, gw_ref, tok_ref, cot_ref, out_ref):
    code, first, second = slot_codes(rt_ref[...])
    gw = gw_ref[...]
    weight = jnp.where(first, gw[0:1, :], 0.0) + jnp.where(second, gw[1:2, :], 0.0)
    shape = (EXPERTS, PAIR, TOK)
    code3 = jnp.broadcast_to(code[:, None, :], shape)
    weight3 = jnp.broadcast_to(weight[:, None, :], shape)
    at = iota(shape, 1)
    atf = at.astype(F32)
    sel_x = jnp.where(code3 == atf, jnp.where(at < CAP, 1.0, 0.0), 0.0)
    sel_g = jnp.where(code3 == atf - float(CAP), jnp.where(at >= CAP, 1.0, 0.0), 0.0)
    scale = jnp.sum(sel_g * weight3 + sel_x, axis=2, keepdims=True).reshape(ROWS, 1)
    select = jnp.concatenate(
        [sel_x.reshape(ROWS, TOK).astype(BF16), sel_g.reshape(ROWS, TOK).astype(BF16)], axis=1
    )
    source = jnp.concatenate([tok_ref[...], cot_ref[...]], axis=0)
    rows = jnp.dot(select, source, preferred_element_type=F32)
    out_ref[...] = (rows * scale).astype(BF16).reshape(EXPERTS, PAIR, WIDTH)


def dispatch(rt, gw, tokens, cotangent):
    out = (pltpu.VMEM((EXPERTS, PAIR, WIDTH), BF16),)
    return kernel_call(dispatch_kernel, out, "dispatch", rt, gw, tokens, cotangent)[0]


def vmem(value):
    return pltpu.with_memory_space_constraint(value, pltpu.VMEM)


def kernel_call(body, out, name, *values, core=None, scratch=(), far=(), near=(), far_out=0):
    specs = [pl.BlockSpec(memory_space=pl.ANY)] * len(far)
    specs += [pl.BlockSpec(memory_space=pltpu.VMEM)] * len(near)
    specs += [pl.BlockSpec()] * len(values)
    values = [*far, *(vmem(v) for v in near), *values]
    if core is not None:
        specs, values = [pl.BlockSpec(memory_space=pltpu.SMEM)] + specs, [core] + values
    results = [
        pl.BlockSpec(memory_space=pl.ANY)
        if at < far_out
        else pl.BlockSpec()
        if isinstance(shape, jax.ShapeDtypeStruct)
        else pl.BlockSpec(memory_space=pltpu.VMEM)
        for at, shape in enumerate(out)
    ]
    return pl.pallas_call(
        body,
        in_specs=specs,
        out_specs=results,
        out_shape=list(out),
        scratch_shapes=list(scratch),
        name=name,
    )(*values)


def fetch(pairs, sems):
    copies = [
        pltpu.make_async_copy(there, here, sems.at[at]) for at, (there, here) in enumerate(pairs)
    ]
    for copy in copies:
        copy.start()
    return copies


def flags(count):
    return pltpu.SemaphoreType.DMA((count,))


def lanes_of(step, half):
    return pl.ds(pl.multiple_of((2 * step + half) * WIDTH, WIDTH), WIDTH)


def half_lanes(y):
    return slice(y * WIDTH, (y + 1) * WIDTH)


def split_kernel(c_ref, wg_ref, wu_ref, wd_ref, out_ref):
    for at, ref in enumerate((wg_ref, wu_ref, wd_ref)):
        for y in range(NY):
            out_ref[at, :, half_lanes(y)] = ref[:, lanes_of(y, 1 - c_ref[0])]


def other_half(core, wg, wu, wd):
    out = (jax.ShapeDtypeStruct((3, HID, HALF), BF16),)
    return kernel_call(split_kernel, out, "other_half", wg, wu, wd, core=core)[0]


def is_token_lane(shape):
    lane = iota(shape, 1)
    return lane - ((lane * 2731) >> 16) * PAIR < CAP


def forward_kernel(
    c_ref, xg_far, wg_far, wu_far, wd_far, wr_ref, out_ref, xg_ref, own_ref, sems
):
    pairs = []
    for y in range(NY):
        pairs.append((xg_far.at[y], xg_ref.at[y]))
        for at, far in enumerate((wg_far, wu_far, wd_far)):
            pairs.append((far.at[:, lanes_of(y, c_ref[0])], own_ref.at[at, :, half_lanes(y)]))
    copies = fetch(pairs, sems)
    total = None
    for y in range(NY):
        for copy in copies[4 * y : 4 * y + 4]:
            copy.wait()
        parts = []
        for at in (0, 2, 1):
            parts.append(own_ref[at, :, half_lanes(y)])
            parts.append(wr_ref[at, :, half_lanes(y)])
        part = lax.dot_general(
            jnp.concatenate(parts, axis=0),
            xg_ref[y],
            (((1,), (1,)), ((), ())),
            preferred_element_type=F32,
        )
        total = part if total is None else total + part
    pair = 2 * HID
    out_ref[0:pair, :] = jnp.where(
        is_token_lane((pair, ROWS)), total[0:pair, :], total[pair : 2 * pair, :]
    ).astype(BF16)
    out_ref[pair : 2 * pair, :] = total[2 * pair : 3 * pair, :].astype(BF16)


def forward(core, xg, wg, wu, wd, wr):
    out = (pltpu.VMEM((4 * HID, ROWS), BF16),)
    return kernel_call(
        forward_kernel,
        out,
        "forward",
        core=core,
        far=(xg, wg, wu, wd),
        near=(wr,),
        scratch=(
            pltpu.VMEM((NY, ROWS, WIDTH), BF16),
            pltpu.VMEM((3, HID, HALF), BF16),
            flags(4 * NY),
        ),
    )[0]


def backward_kernel(
    c_ref, wg_far, wu_far, wr_ref, own_ref, got_ref, out_far, left_far,
    wg_ref, wu_ref, out_ref, left_ref, sems, out_sems,
):
    copies = fetch(
        [
            (wg_far, wg_ref),
            (wu_far, wu_ref),
        ],
        sems,
    )

    def total(at):
        low, mid, high = 2 * at * HID, (2 * at + 1) * HID, (2 * at + 2) * HID
        return jnp.concatenate(
            [
                own_ref[low:mid, :].astype(F32) + got_ref[mid:high, :].astype(F32),
                own_ref[mid:high, :].astype(F32) + got_ref[low:mid, :].astype(F32),
            ],
            axis=0,
        )

    pre_gate, pre_up = total(0), total(1)
    keep = is_token_lane((2 * HID, ROWS))
    back = pltpu.roll(pre_gate, ROWS - CAP, 1)
    sig = 1.0 / (1.0 + jnp.exp(-jnp.where(keep, pre_gate, 0.0)))
    silu = pre_gate * sig
    hidden = jnp.where(keep, silu * pre_up, 0.0).astype(BF16).astype(F32)
    grad_gate = jnp.where(keep, back * pre_up * sig * (1.0 + pre_gate * (1.0 - sig)), 0.0)
    grad_up = jnp.where(keep, back * silu, 0.0)
    gate = jnp.sum(hidden * back, axis=0, keepdims=True)
    upper = gate.astype(BF16).astype(F32)
    tail = [part[:, half_lanes(at)] for part in (upper, gate - upper) for at in range(3)]
    tail = jnp.concatenate(tail + [jnp.zeros((2, WIDTH), F32)], axis=0).astype(BF16)
    shifted = pltpu.roll(hidden, CAP, 1)
    for at, grad in enumerate((grad_gate, grad_up, shifted)):
        grad = grad.astype(BF16)
        left_ref[0, at * HID : (at + 1) * HID, :] = grad[0:HID]
        left_ref[1, at * HID : (at + 1) * HID, :] = grad[HID : 2 * HID]
    sent = [pltpu.make_async_copy(left_ref, left_far, out_sems.at[NY])]
    sent[0].start()
    both = jnp.concatenate([grad_gate.astype(BF16), grad_up.astype(BF16)], axis=0)
    slot = iota((SLOTS, ROWS), 0)
    lane = iota((SLOTS, ROWS), 1)
    compact = jnp.where(lane == slot + ((slot * 5462) >> 16) * CAP, 1.0, 0.0).astype(BF16)
    grads = lax.dot_general(
        compact, both, (((1,), (1,)), ((), ())), preferred_element_type=F32
    ).astype(BF16)
    for copy in copies:
        copy.wait()
    for y in range(NY):
        mats = jnp.concatenate(
            [
                wg_ref[:, lanes_of(y, c_ref[0])],
                wr_ref[0, :, half_lanes(y)],
                wu_ref[:, lanes_of(y, c_ref[0])],
                wr_ref[1, :, half_lanes(y)],
            ],
            axis=0,
        )
        out_ref[y, 0:SLOTS, :] = jnp.dot(grads, mats, preferred_element_type=F32).astype(BF16)
        out_ref[y, SLOTS:BACK, :] = tail
        sent.append(pltpu.make_async_copy(out_ref.at[y], out_far.at[y], out_sems.at[y]))
        sent[-1].start()
    for copy in sent:
        copy.wait()


def backward(core, own, got, wg, wu, wr):
    out = (
        jax.ShapeDtypeStruct((NY, BACK, WIDTH), BF16),
        jax.ShapeDtypeStruct((2, 3 * HID, ROWS), BF16),
    )
    return kernel_call(
        backward_kernel,
        out,
        "backward",
        core=core,
        far=(wg, wu),
        near=(wr, own, got),
        far_out=2,
        scratch=(
            pltpu.VMEM((HID, 2 * HALF), BF16),
            pltpu.VMEM((HID, 2 * HALF), BF16),
            pltpu.VMEM((NY, BACK, WIDTH), BF16),
            pltpu.VMEM((2, 3 * HID, ROWS), BF16),
            flags(2),
            flags(NY + 1),
        ),
    )


def partner_kernel(left_far, xg_far, out_ref, left_ref, xg_ref, sems):
    copies = fetch(
        [(left_far.at[1], left_ref)] + [(xg_far.at[y], xg_ref.at[y]) for y in range(NY)], sems
    )
    copies[0].wait()
    for y in range(NY):
        copies[1 + y].wait()
        out_ref[:, half_lanes(y)] = jnp.dot(
            left_ref[...], xg_ref[y], preferred_element_type=F32
        ).astype(BF16)


def partner_grads(left, xg):
    return kernel_call(
        partner_kernel,
        (jax.ShapeDtypeStruct((3 * HID, HALF), BF16),),
        "partner_grads",
        far=(left, xg),
        scratch=(
            pltpu.VMEM((3 * HID, ROWS), BF16),
            pltpu.VMEM((NY, ROWS, WIDTH), BF16),
            flags(1 + NY),
        ),
    )[0]


def merge_kernel(
    c_ref, left_far, xg_far, got_far, gate_far, up_far, down_far, left_ref, xg_ref, got_ref, out_ref, sems, out_sems
):
    copies = fetch(
        [(left_far.at[0], left_ref), (got_far, got_ref)]
        + [(xg_far.at[y], xg_ref.at[y]) for y in range(NY)],
        sems,
    )
    copies[0].wait()
    copies[1].wait()
    sent = []
    for y in range(NY):
        copies[2 + y].wait()
        mine = jnp.dot(left_ref[...], xg_ref[y], preferred_element_type=F32)
        theirs = got_ref[:, half_lanes(y)].astype(F32)
        both = slice(2 * y * WIDTH, (2 * y + 2) * WIDTH)
        for at, far in enumerate((gate_far, up_far, down_far)):
            rows = slice(at * HID, (at + 1) * HID)
            out_ref[at, :, lanes_of(y, c_ref[0])] = mine[rows, :]
            out_ref[at, :, lanes_of(y, 1 - c_ref[0])] = theirs[rows, :]
            sent.append(
                pltpu.make_async_copy(
                    out_ref.at[at, :, both], far.at[:, both], out_sems.at[3 * y + at]
                )
            )
            sent[-1].start()
    for copy in sent:
        copy.wait()


def merged_grads(core, left, xg, got):
    return kernel_call(
        merge_kernel,
        [jax.ShapeDtypeStruct((HID, 2 * HALF), F32)] * 3,
        "merged_grads",
        core=core,
        far=(left, xg, got),
        far_out=3,
        scratch=(
            pltpu.VMEM((3 * HID, ROWS), BF16),
            pltpu.VMEM((NY, ROWS, WIDTH), BF16),
            pltpu.VMEM((3 * HID, HALF), BF16),
            pltpu.VMEM((3, HID, 2 * HALF), F32),
            flags(2 + NY),
            flags(3 * NY),
        ),
    )


def place_kernel(got_ref, out_ref):
    total = got_ref[...].astype(F32)
    gate = total[SLOTS : SLOTS + 3, :] + total[SLOTS + 3 : SLOTS + 6, :]
    gate = jnp.concatenate([gate[at : at + 1, :] for at in range(3)], axis=1)
    total = total[0:SLOTS, :].astype(BF16)
    src = iota((EXPERTS, ROWS), 0)
    lane = iota((EXPERTS, ROWS), 1)
    table = jnp.where(
        (lane * 2731) >> 16 == src, jnp.broadcast_to(gate, (EXPERTS, ROWS)), 0.0
    ).astype(BF16)
    at = iota((ROWS, WIDTH), 0)
    picks = jnp.where(
        at - ((at * 2731) >> 16) * PAIR == iota((ROWS, WIDTH), 1), 1.0, 0.0
    ).astype(BF16)
    shares = jnp.dot(table, picks, preferred_element_type=F32).astype(BF16)
    row = iota((EXPERTS * 16, SLOTS + EXPERTS), 0)
    col = iota((EXPERTS * 16, SLOTS + EXPERTS), 1)
    source = row >> 4
    want = jnp.where(
        row - source * 16 < CAP,
        source * CAP + row - source * 16,
        jnp.where(row - source * 16 == CAP, SLOTS + source, -1),
    )
    place = jnp.where(col == want, 1.0, 0.0).astype(BF16)
    rows = jnp.dot(
        place, jnp.concatenate([total, shares], axis=0), preferred_element_type=F32
    )
    out_ref[...] = rows.astype(BF16).reshape(EXPERTS, 16, WIDTH)


def placed_rows(got):
    out = (pltpu.VMEM((EXPERTS, 16, WIDTH), BF16),)
    return kernel_call(place_kernel, out, "placed_rows", got)[0]


def combine_kernel(back_ref, rt_ref, gw_ref, out_ref, gate_ref):
    code, first, second = slot_codes(rt_ref[...])
    shape = (EXPERTS, 16, TOK)
    code3 = jnp.broadcast_to(code[:, None, :], shape)
    select = jnp.where(code3 == iota(shape, 1).astype(F32), 1.0, 0.0)
    select = select.reshape(EXPERTS * 16, TOK).T.astype(BF16)
    back = back_ref[...]
    rows = jnp.dot(
        select, back.reshape(EXPERTS * 16, WIDTH), preferred_element_type=F32
    )
    out_ref[...] = rows.astype(BF16)
    shares = back[:, CAP, 0:TOK].astype(F32)
    mine = jnp.zeros((EXPERTS, TOK), F32)
    for p in range(CAP):
        mine = mine + jnp.where(code == float(p), shares[:, p : p + 1], 0.0)
    top = jnp.sum(jnp.where(first, mine, 0.0), axis=0, keepdims=True)
    low = jnp.sum(jnp.where(second, mine, 0.0), axis=0, keepdims=True)
    gate_ref[...] = jnp.concatenate([top, low], axis=0) / gw_ref[...]


def combine(rt, gw, back):
    out = (
        jax.ShapeDtypeStruct((TOK, WIDTH), BF16),
        jax.ShapeDtypeStruct((TOP, TOK), F32),
    )
    return kernel_call(combine_kernel, out, "combine", near=(back, rt, gw))


def core_swap(value):
    return lax.ppermute(value, "c", [(0, 1), (1, 0)])


def shards(tokens, cotangent, routes, gate_weight, w_gate, w_up, w_down, shared_hidden):
    rt, gw = routes.T, gate_weight.T
    core = lax.axis_index("c").astype(I32).reshape(1)
    wg, wu, wd = w_gate[0], w_up[0], w_down[0]
    sent = dispatch(rt, gw, tokens, cotangent)
    rows = lax.all_to_all(sent, EP, split_axis=0, concat_axis=0, tiled=True)
    rows, cotangent, wg, wu, wd = lax.optimization_barrier((rows, cotangent, wg, wu, wd))
    xg = lax.all_gather(rows.reshape(ROWS, WIDTH), "y", axis=0, tiled=False)

    wr = core_swap(other_half(core, wg, wu, wd))
    shared = lax.dot_general(
        shared_hidden, cotangent, (((0,), (0,)), ((), ())), preferred_element_type=F32
    ).astype(BF16)
    shared = lax.all_to_all(
        shared.reshape(EXPERTS, -1, WIDTH), EP, split_axis=0, concat_axis=0, tiled=True
    )
    shared_grad = jnp.sum(shared.astype(F32), axis=0)
    xg, wr, shared_grad = lax.optimization_barrier((xg, wr, shared_grad))

    own = forward(core, xg, wg, wu, wd, wr)
    parts, left = backward(core, own, core_swap(own), wg, wu, wr)
    got = lax.psum_scatter(parts, "y", scatter_dimension=0, tiled=False)
    theirs = core_swap(partner_grads(left, xg))
    grads = merged_grads(core, left, xg, theirs)
    got, *grads = lax.optimization_barrier((got, *grads))
    back = lax.all_to_all(placed_rows(got), EP, split_axis=0, concat_axis=0, tiled=True)
    tokens_grad, gate_grad = combine(rt, gw, back)
    return (tokens_grad, gate_grad.T, grads[0][None], grads[1][None], grads[2][None], shared_grad)


def solution(mesh):
    split = Mesh(mesh.devices.reshape(8, 4, 8, 2), ("z", "x", "y", "c"))
    ep, tp = ("z", "x"), ("y", "c")
    placed = (
        P(ep, tp),
        P(ep, tp),
        P(ep, None),
        P(ep, None),
        P(ep, tp, None),
        P(ep, tp, None),
        P(ep, tp, None),
        P(ep, None),
    )
    return jax.shard_map(
        shards,
        mesh=split,
        in_specs=placed,
        out_specs=(
            P(ep, tp),
            P(ep, None),
            P(ep, tp, None),
            P(ep, tp, None),
            P(ep, tp, None),
            P(ep, tp),
        ),
        check_vma=False,
    )
```
